32 devices in a mesh: fs: 8 (over z, y), tp: 4 (over x, core).
Axes of the slice: x: 2, y: 2, z: 4, core: 2. Of those that a mesh axis runs over, the one named last changes fastest.
Arguments:
- tokens: bfloat16 [8192, 2048], P('fs', 'tp'), may hold values from -6 to 6
- norm_gain: float32 [2048], P('fs'), may hold values from 0.1 to 1.9
- up_master: float32 [2048, 4096], P('fs', 'tp'), may hold values from -0.125 to 0.125
- down_master: float32 [4096, 2048], P('fs', 'tp'), may hold values from -0.09375 to 0.09375
Outputs:
- mixed: bfloat16 [8192, 2048], P('fs', 'tp')
- up_ready: bfloat16 [2048, 4096], P(None, 'tp')
- down_ready: bfloat16 [4096, 2048], P('tp')
The draws below stay inside these ranges and needn't reach their ends.
All inputs are finite; a program needn't handle non-finite values.
Results may differ from the reference program's by a relative error of at most 0.0095.
Values may be sent and summed in bfloat16 or wider, within the bound.
A program may use at most 128 MiB of HBM per device.

```python
import jax
import jax.numpy as jnp
from jax import lax

D = 2048
FF = 4096
TOKENS = 8192
N_TP = 4


def steps_of(key, shape, shards, least, high):
    factor_of, own = 1.0, jax.random.fold_in(key, 6)
    for axis_at, blocks in shards:
        steps = jnp.exp(jax.random.uniform(jax.random.fold_in(own, axis_at), (blocks,), jnp.float32, least / len(shards), high / len(shards)))
        factor_of = factor_of * jnp.repeat(steps, shape[axis_at] // blocks).reshape([-1 if axis == axis_at else 1 for axis in range(len(shape))])
    return factor_of


def gaussian(rng, dims, spread, bound, pieces=(), held_as=jnp.bfloat16):
    loudness = steps_of(rng, dims, pieces, -0.22, 0.18) if pieces else 1.0
    array = jax.random.normal(rng, dims, jnp.float32) * spread * loudness
    return jnp.minimum(jnp.maximum(array, -bound), bound).astype(held_as)


def setup_inputs(seed: int = 0) -> dict:
    arg_keys = jax.random.split(jax.random.key(seed), 5)
    tokens = gaussian(arg_keys[0], (TOKENS, D), 1.0, 6.0, ((0, 8), (1, 4)))
    norm_gain = jnp.clip(1.0 + 0.18 * jax.random.normal(arg_keys[1], (D,), jnp.float32), 0.1, 1.9)
    up_master = gaussian(arg_keys[2], (D, FF), D ** -0.5, 0.125, ((0, 8), (1, 4)), jnp.float32)
    down_master = gaussian(arg_keys[3], (FF, D), FF ** -0.5, 0.09375, ((0, 8), (1, 4)), jnp.float32)
    return {"tokens": tokens, "norm_gain": norm_gain, "up_master": up_master, "down_master": down_master}


def reference(tokens, norm_gain, up_master, down_master):
    up_ready = (norm_gain[:, None] * up_master).astype(jnp.bfloat16)
    down_ready = down_master.astype(jnp.bfloat16)
    values = tokens.astype(jnp.float32)
    mean_square = lax.optimization_barrier(jnp.mean(values * values, axis=-1, keepdims=True))
    normed = (values * lax.rsqrt(mean_square + 1e-06)).astype(jnp.bfloat16)
    before = jnp.dot(normed, up_ready, preferred_element_type=jnp.float32)
    hidden = jnp.square(jax.nn.relu(before)).astype(jnp.bfloat16)
    block_size = FF // N_TP
    total = jnp.zeros((tokens.shape[0], D), jnp.float32)
    for block_id in range(N_TP):
        first = block_id * block_size
        partial_value = jnp.dot(hidden[:, first:first + block_size], down_ready[first:first + block_size], preferred_element_type=jnp.float32).astype(jnp.bfloat16)
        partial_value = lax.optimization_barrier(partial_value)
        total = total + partial_value.astype(jnp.float32)
    return (total.astype(jnp.bfloat16), up_ready, down_ready)
```

```python
import functools

import jax
import jax.numpy as jnp
from jax import lax
from jax.experimental import pallas as pl
from jax.experimental.pallas import tpu as pltpu
from jax.sharding import PartitionSpec as P

UP_CUTS = 2
DOWN_CUTS = 2
COLUMNS = 256
BOTH = 3
LANES = 128
VMEM_LIMIT = 40
MIB = 1024 * 1024


def kernel(
    n, n_tp,
    tokens_hbm, gain_hbm, upm_hbm, downm_hbm,
    up, down, own, take, crossed,
    gain_in, upm_in, downm_in, tok, shard, passing, scale, hidden, kept, give, cross,
    tok_send, tok_recv, gather_send, gather_recv,
    up_send, upz_recv, upy_recv, both_send, both_recv,
    down_send, downz_recv, downy_recv, pass_send, pass_recv, last_send, last_recv,
    pair_send, pair_recv, cross_send, cross_recv, local_sem,
):
    f32, bf16 = jnp.float32, jnp.bfloat16
    f, t = lax.axis_index("fs"), lax.axis_index("tp")
    lines = n // 2
    z, y = f // 2, f % 2
    t1 = t + 1 - 2 * (t % 2)
    t2 = (t + 2) % 4
    t3 = (t1 + 2) % 4
    members = n // n_tp
    starts = members // 2
    owner = f // members
    above, below = (f + 2) % n, (f + n - 2) % n
    across = f + 1 - 2 * y
    has_above, has_below = z < lines - 1, z > 0
    upper, lower = t >= n_tp // 2, t < n_tp // 2
    at_end = jnp.logical_not(has_above & has_below)

    up_rows = upm_in.shape[0]
    down_rows = downm_in.shape[0]
    feats = tokens_hbm.shape[1]
    half = feats // 2
    dcut = down_rows // DOWN_CUTS
    first_cut = max(8, up_rows * BOTH // 128 * 8)
    ucuts = (first_cut, first_cut + (up_rows - first_cut) // 16 * 8, up_rows)

    def remote(src, dst, send, recv, **to):
        return pltpu.make_async_remote_copy(
            src_ref=src, dst_ref=dst, send_sem=send, recv_sem=recv,
            device_id=to, device_id_type=pl.DeviceIdType.MESH,
        )

    def down_block(source, column):
        rows = pl.ds(pl.multiple_of(source % members * down_rows, down_rows), down_rows)
        return down.at[rows, pl.ds(pl.multiple_of(column * feats, feats), feats)]

    loads = [
        pltpu.make_async_copy(upm_hbm, upm_in, local_sem.at[0]),
        pltpu.make_async_copy(gain_hbm, gain_in, local_sem.at[1]),
        pltpu.make_async_copy(downm_hbm, downm_in, local_sem.at[2]),
        pltpu.make_async_copy(
            tokens_hbm, tok.at[:, pl.ds(pl.multiple_of(t * feats, feats), feats)],
            local_sem.at[3],
        ),
    ]
    for load in loads:
        load.start()

    barrier = pltpu.get_barrier_semaphore()
    for other in (t1, t2, t3):
        pl.semaphore_signal(
            barrier, inc=1, device_id={"tp": other}, device_id_type=pl.DeviceIdType.MESH
        )
    pl.semaphore_signal(
        barrier, inc=1, device_id={"fs": across}, device_id_type=pl.DeviceIdType.MESH
    )

    @pl.when(has_above)
    def _():
        pl.semaphore_signal(
            barrier, inc=1, device_id={"fs": above}, device_id_type=pl.DeviceIdType.MESH
        )

    @pl.when(has_below)
    def _():
        pl.semaphore_signal(
            barrier, inc=1, device_id={"fs": below}, device_id_type=pl.DeviceIdType.MESH
        )

    loads[0].wait()
    loads[1].wait()
    gain = jnp.transpose(jnp.broadcast_to(gain_in[...], (LANES, up_rows)))
    for first in range(0, up.shape[1], LANES):
        up[pl.ds(pl.multiple_of(f * up_rows, up_rows), up_rows), pl.ds(first, LANES)] = (
            gain * upm_in[:, pl.ds(first, LANES)]
        ).astype(bf16)

    loads[2].wait()

    @pl.when(owner == t)
    def _():
        down_block(f, t)[...] = downm_in[...].astype(bf16)

    @pl.when(owner == t2)
    def _():
        passing[z % starts] = downm_in[...].astype(bf16)

    @pl.when((owner == t1) | (owner == t3))
    def _():
        shard[...] = downm_in[...].astype(bf16)

    pl.semaphore_wait(
        barrier, 4 + has_above.astype(jnp.int32) + has_below.astype(jnp.int32)
    )

    def up_piece(line, column, u):
        first, last = (ucuts[u], ucuts[u + 1]) if u >= 0 else (0, ucuts[0])
        row = (line * 2 + column) * up_rows + first
        return up.at[pl.ds(pl.multiple_of(row, 8), last - first), :]

    def both_copy(way, line, column, to):
        piece = up_piece(line, column, -1)
        return remote(
            piece, piece, both_send.at[way, line, column], both_recv.at[line, column], fs=to
        )

    def run(copy, start):
        copy.start() if start else copy.wait_send()

    def both_onward(line, column, start):
        @pl.when(has_above & (line <= z))
        def _():
            run(both_copy(0, line, column, above), start)

        @pl.when(has_below & (line >= z))
        def _():
            run(both_copy(1, line, column, below), start)

    def up_copy(way, line, u, to):
        piece = up_piece(line, y, u)
        recv = upy_recv if way == 2 else upz_recv
        return remote(piece, piece, up_send.at[way, line, u], recv.at[line, u], fs=to)

    def up_onward(line, u, start):
        @pl.when(has_above & (line <= z))
        def _():
            run(up_copy(0, line, u, above), start)

        @pl.when(has_below & (line >= z))
        def _():
            run(up_copy(1, line, u, below), start)

        run(up_copy(2, line, u, across), start)

    both_copy(2, z, y, across).start()
    both_onward(z, y, True)
    for u in range(UP_CUTS):
        up_onward(z, u, True)

    def gather_copy(column, to):
        return remote(
            shard, down_block(f, column), gather_send.at[0], gather_recv.at[column], tp=to
        )

    order = ((t3, 0), (t2, 0), (t3, 1), (t2, 1), (t1, 0), (t1, 1), (t, 0), (t, 1))
    passed = (1, 3)
    finals = 7
    early = (0, 1, 2)

    def pass_copies(part, js, q, start, ways=(0, 1)):
        line = t2 * starts + js
        row = ((line * 2 + y) % members) * down_rows + q * dcut
        ci = passed[part]
        here = passing.at[js, pl.ds(q * dcut, dcut), pl.ds(part * half, half)]
        there = down.at[
            pl.ds(pl.multiple_of(row, dcut), dcut),
            pl.ds(pl.multiple_of(t * feats + part * half, half), half),
        ]

        def onward(to):
            return remote(
                here, here, pass_send.at[0, part, js, q], pass_recv.at[part, js, q], fs=to
            )

        if 0 in ways:
            @pl.when(lower & has_below & (line >= z))
            def _():
                run(onward(below), start)

            @pl.when(upper & has_above & (line <= z))
            def _():
                run(onward(above), start)

        if 1 in ways:
            @pl.when((upper & (line <= z)) | (lower & (line >= z)))
            def _():
                over = remote(
                    here, there, pass_send.at[1, part, js, q], downz_recv.at[ci, js, q],
                    tp=t2,
                )
                run(over, start)

    def pass_on(part, q):
        @pl.loop(0, starts)
        def _(js):
            line = t2 * starts + js

            @pl.when((upper & (line < z)) | (lower & (line > z)))
            def _():
                here = passing.at[js, pl.ds(q * dcut, dcut), pl.ds(part * half, half)]
                remote(
                    here, here, pass_send.at[0, part, js, q], pass_recv.at[part, js, q],
                    fs=above,
                ).wait_recv()
                pass_copies(part, js, q, True)

    def pass_start(way):
        @pl.when(owner == t2)
        def _():
            for part in range(2):
                for q in range(DOWN_CUTS):
                    pass_copies(part, z % starts, q, True, (way,))

    @pl.when((owner == t1) | (owner == t3))
    def _():
        gather_copy(t, owner).start()

    pass_start(1)
    loads[3].wait()

    def tok_copy(way, column, to):
        piece = tok.at[:, pl.ds(pl.multiple_of(column * feats, feats), feats)]
        return remote(piece, piece, tok_send.at[way], tok_recv.at[way], tp=to)

    tok_copy(1, t, t2).start()
    tok_copy(0, t, t1).start()

    both_copy(2, z, 1 - y, across).wait_recv()
    both_onward(z, 1 - y, True)

    def both_relay(line, column):
        @pl.when((line >= 0) & (line < lines))
        def _():
            both_copy(0, line, column, above).wait_recv()
            both_onward(line, column, True)

    def down_piece(ci, js, side, q):
        column, part = order[ci]
        line = t * starts + js
        row = ((line * 2 + side) % members) * down_rows + q * dcut
        return down.at[
            pl.ds(pl.multiple_of(row, dcut), dcut),
            pl.ds(pl.multiple_of(column * feats + part * half, half), half),
        ]

    def down_copy(way, ci, js, q, to):
        piece = down_piece(ci, js, y, q)
        recv = downy_recv if way == 2 else downz_recv
        return remote(
            piece, piece, down_send.at[way, ci, js, q], recv.at[ci, js, q], fs=to
        )

    def down_lines(ci, js, q, start):
        line = t * starts + js
        rising = has_above & (line <= z)
        falling = has_below & (line >= z)
        if ci in passed:
            rising = rising & upper
            falling = falling & lower
        elif start:
            rising = rising & (upper | (line < z))
            falling = falling & (lower | (line > z))

        @pl.when(rising)
        def _():
            run(down_copy(0, ci, js, q, above), start)

        @pl.when(falling)
        def _():
            run(down_copy(1, ci, js, q, below), start)

    def down_over(ci, js, q, start):
        line = t * starts + js
        if ci == finals:
            @pl.when(line == z)
            def _():
                run(down_copy(2, ci, js, q, across), start)
        elif start and ci in early:
            @pl.when(line != z)
            def _():
                down_copy(2, ci, js, q, across).start()
        else:
            run(down_copy(2, ci, js, q, across), start)

    def far_start():
        js = z % starts

        def send(make):
            @pl.when(lower & has_above)
            def _():
                make(0, above).start()

            @pl.when(upper & has_below)
            def _():
                make(1, below).start()

        @pl.when(owner == t)
        def _():
            for ci in (0, 2, 4, 5, 6):
                for q in range(DOWN_CUTS):
                    send(lambda way, to: down_copy(way, ci, js, q, to))
            for q in range(DOWN_CUTS):
                send(lambda way, to: last_copy(way, js, y, q, to))

    def last_copy(way, js, side, q, to):
        piece = down_piece(finals, js, side, q)
        return remote(
            piece, piece, last_send.at[way, js, side, q], last_recv.at[js, side, q], fs=to
        )

    def last_onward(js, side, q, start, sent=False):
        line = t * starts + js
        rising = has_above & (line <= z)
        falling = has_below & (line >= z)
        if sent:
            rising = rising & (upper | (line < z))
            falling = falling & (lower | (line > z))

        @pl.when(rising)
        def _():
            run(last_copy(0, js, side, q, above), start)

        @pl.when(falling)
        def _():
            run(last_copy(1, js, side, q, below), start)

    def relay(ci, q, ways=(0, 1)):
        @pl.loop(0, starts)
        def _(js):
            if 0 in ways:
                if ci in passed and ci not in early:
                    down_copy(0, ci, js, q, above).wait_recv()
                else:
                    @pl.when(t * starts + js != z)
                    def _():
                        down_copy(0, ci, js, q, above).wait_recv()

                down_lines(ci, js, q, True)
            if 1 in ways:
                down_over(ci, js, q, True)

    def relay_line(ci, q):
        relay(ci, q, (0,))

    def relay_over(ci, q):
        relay(ci, q, (1,))

    def last_start():
        @pl.loop(0, starts)
        def _(js):
            for q in range(DOWN_CUTS):
                down_over(finals, js, q, True)

    def last_turn():
        @pl.when(owner == t)
        def _():
            js = z % starts
            for q in range(DOWN_CUTS):
                piece = down_piece(finals, js, 1 - y, q)
                remote(
                    piece, piece, down_send.at[2, finals, js, q],
                    downy_recv.at[finals, js, q], fs=across,
                ).wait_recv()
                last_onward(js, 1 - y, q, True)
                last_onward(js, y, q, True, True)

    def last_relay(side, q):
        @pl.loop(0, starts)
        def _(js):
            @pl.when(t * starts + js != z)
            def _():
                last_copy(0, js, side, q, above).wait_recv()
                last_onward(js, side, q, True, True)

    def relayed(ci):
        @pl.loop(0, starts)
        def _(js):
            for q in range(DOWN_CUTS):
                piece = down_piece(ci, js, 1 - y, q)
                remote(
                    piece, piece, down_send.at[2, ci, js, q], downy_recv.at[ci, js, q],
                    fs=across,
                ).wait_recv()

    @pl.when(owner == t)
    def _():
        for ci in (4, 0):
            gather_copy(order[ci][0], t).wait_recv()

    @pl.when(at_end)
    def _():
        pass_start(0)
        far_start()

    @pl.loop(1, lines)
    def _(d):
        both_relay(z - d, y)
        both_relay(z + d, y)
        for u in range(UP_CUTS):
            @pl.when(z - d >= 0)
            def _():
                up_copy(0, z - d, u, above).wait_recv()
                up_onward(z - d, u, True)

            @pl.when(z + d < lines)
            def _():
                up_copy(1, z + d, u, below).wait_recv()
                up_onward(z + d, u, True)

        both_relay(z - d, 1 - y)
        both_relay(z + d, 1 - y)

        for k in range(len(early)):
            @pl.when((owner == t) & (d == k + 1))
            def _():
                for q in range(DOWN_CUTS):
                    if early[k] in passed:
                        down_copy(0, early[k], z % starts, q, above).wait_recv()
                    down_copy(2, early[k], z % starts, q, across).start()

    @pl.when(has_above & has_below)
    def _():
        pass_start(0)
        far_start()

    last_start()
    inside = has_above & has_below
    near = (lower & (z < lines // 2)) | (upper & (z >= lines // 2))
    far = jnp.logical_not(near)

    def when(condition, *moves):
        @pl.when(condition)
        def _():
            for move, which, cuts in moves:
                for q in cuts:
                    move(which, q)

    every = range(DOWN_CUTS)
    when(inside, (pass_on, 0, every))

    def share():
        tok_copy(1, t2, t2).wait_recv()
        tok_copy(2, t2, t1).start()

    pl.when(inside)(share)
    when(inside, (relay, 0, every))
    when(inside & near, (relay, 1, every))
    when(inside, (pass_on, 1, every), (relay, 2, every))
    when(inside & near, (relay, 3, every), *((relay_line, ci, every) for ci in (4, 5, 6)))
    pl.when(at_end)(share)
    when(at_end & far, (relay, 0, every[:1]))
    when(at_end & near, (pass_on, 0, every[:1]))
    tok_copy(0, t1, t1).wait_recv()
    tok_copy(2, t3, t1).wait_recv()

    rows_all = tok.shape[0]
    step = min(rows_all, 128)

    @pl.loop(0, rows_all // step)
    def _(i):
        rows = pl.ds(pl.multiple_of(i * step, step), step)
        values = tok[rows, :].astype(f32)
        mean_square = jnp.mean(values * values, axis=-1, keepdims=True)
        scale[rows, :] = lax.rsqrt(mean_square + 1e-06)

    @pl.loop(0, lines)
    def _(line):
        for u in range(UP_CUTS):
            piece = up_piece(line, 1 - y, u)
            remote(
                piece, piece, up_send.at[2, line, u], upy_recv.at[line, u], fs=across
            ).wait_recv()

    width = up.shape[1]
    tiles = width // COLUMNS
    steps = 4
    for k in range(steps):
        @pl.loop(k * tiles // steps, (k + 1) * tiles // steps)
        def _(i):
            columns = pl.ds(pl.multiple_of(i * COLUMNS, COLUMNS), COLUMNS)
            before = jnp.dot(tok[...], up[:, columns], preferred_element_type=f32)
            value = jnp.maximum(before * scale[...], 0.0)
            hidden[:, columns] = (value * value).astype(bf16)

        when(inside & far, (relay_line, 4 + k // 2, every[k % 2 :: 2]))
        if k == 0:
            when(at_end & near, (pass_on, 0, every[1:]))
            when(at_end & far, (relay, 0, every[1:]))
        if k == 1:
            when(at_end & near, (relay, 0, every[:1]))
            when(at_end & far, (relay, 1, every[:1]))
        if k == 2:
            when(at_end & near, (relay, 0, every[1:]))
            when(at_end & far, (relay, 2, every[:1]))

    when(at_end & far, (relay, 1, every[1:]), (relay, 2, every[1:]))
    when((at_end & near) | (inside & far), (relay, 1, every))

    def product(ci):
        column, part = order[ci]
        first = pl.multiple_of(column * feats + part * half, half)
        return jnp.dot(hidden[...], down[:, pl.ds(first, half)], preferred_element_type=f32)

    def pair_copy(i):
        return remote(give.at[i], take.at[i], pair_send.at[i], pair_recv.at[i], tp=t1)

    def cross_copy(i):
        return remote(
            cross.at[i], crossed.at[i], cross_send.at[i], cross_recv.at[i], tp=t2
        )

    def cross_over(i):
        pair_copy(i).wait_recv()

        @pl.loop(0, rows_all // step)
        def _(j):
            rows = pl.ds(pl.multiple_of(j * step, step), step)
            cross[i, rows, :] = (kept[rows, :] + take[i, rows, :].astype(f32)).astype(bf16)

        cross_copy(i).start()

    def forward(ci):
        when(at_end, (relay_line, ci, every))
        for q in every:
            relay_over(ci, q)

    relayed(0)
    give[0] = product(0).astype(bf16)
    pair_copy(0).start()
    when(inside & far, (relay_line, 6, every))
    when(at_end & near, (pass_on, 1, every[:1]))
    relayed(1)
    kept[...] = product(1)
    when(at_end & near, (pass_on, 1, every[1:]), (relay, 2, every))
    when(at_end & far, (pass_on, 0, every), (pass_on, 1, every))
    when(at_end | far, (relay, 3, every))
    cross_over(0)
    relayed(2)
    give[1] = product(2).astype(bf16)
    pair_copy(1).start()
    forward(4)
    relayed(3)
    kept[...] = product(3)
    last_turn()
    cross_over(1)
    forward(5)
    forward(6)
    relayed(4)
    give[2] = product(4).astype(bf16)
    pair_copy(2).start()
    last_relay(y, 0)
    last_relay(1 - y, 0)
    relayed(5)
    give[3] = product(5).astype(bf16)
    pair_copy(3).start()
    last_relay(y, 1)
    last_relay(1 - y, 1)
    relayed(6)
    own[0] = product(6)
    own[1] = product(7)
    for i in range(2):
        pair_copy(2 + i).wait_recv()
        cross_copy(i).wait_recv()

    @pl.loop(0, lines)
    def _(line):
        for u in range(UP_CUTS):
            up_onward(line, u, False)
        for column in range(2):
            both_onward(line, column, False)

    both_copy(2, z, y, across).wait_send()

    @pl.loop(0, starts)
    def _(js):
        for q in range(DOWN_CUTS):
            for ci in range(len(order)):
                if ci != finals:
                    down_lines(ci, js, q, False)
                down_over(ci, js, q, False)
            for side in range(2):
                last_onward(js, side, q, False)
            for part in range(2):
                pass_copies(part, js, q, False)

    @pl.when((owner == t1) | (owner == t3))
    def _():
        gather_copy(t, owner).wait_send()

    tok_copy(0, t, t1).wait_send()
    tok_copy(1, t, t2).wait_send()
    tok_copy(2, t2, t1).wait_send()
    for i in range(4):
        pair_copy(i).wait_send()
    for i in range(2):
        cross_copy(i).wait_send()


def finish(up, down, own, take, crossed, mixed_hbm, up_hbm, down_hbm, mixed, sems):
    copies = [
        pltpu.make_async_copy(up, up_hbm, sems.at[0]),
        pltpu.make_async_copy(down, down_hbm, sems.at[1]),
    ]
    for copy in copies:
        copy.start()
    rows_all, half = own.shape[1:]
    step = min(rows_all, 128)
    for i in range(2):
        @pl.loop(0, rows_all // step)
        def _(j):
            rows = pl.ds(pl.multiple_of(j * step, step), step)
            mixed[rows, pl.ds(i * half, half)] = (
                own[i, rows, :] + take[2 + i, rows, :].astype(jnp.float32)
                + crossed[i, rows, :].astype(jnp.float32)
            ).astype(mixed.dtype)

    copies.append(pltpu.make_async_copy(mixed, mixed_hbm, sems.at[2]))
    copies[2].start()
    for copy in copies:
        copy.wait()


def fused(n, n_tp, tokens, norm_gain, up_master, down_master):
    rows, feats = tokens.shape
    up_rows, width = up_master.shape
    down_rows = down_master.shape[0]
    depth = up_rows * n
    model = feats * n_tp
    half = feats // 2
    lines, starts = n // 2, n // n_tp // 2
    bf16, f32 = jnp.bfloat16, jnp.float32
    dma = pltpu.SemaphoreType.DMA
    vmem = pl.BlockSpec(memory_space=pltpu.VMEM)
    hbm = pl.BlockSpec(memory_space=pltpu.HBM)
    flops = 4 * rows * depth * width
    kept = pl.pallas_call(
        functools.partial(kernel, n, n_tp),
        out_shape=(
            pltpu.VMEM((depth, width), bf16),
            pltpu.VMEM((width, model), bf16),
            pltpu.VMEM((2, rows, half), f32),
            pltpu.VMEM((4, rows, half), bf16),
            pltpu.VMEM((2, rows, half), bf16),
        ),
        in_specs=[hbm] * 4,
        out_specs=(vmem,) * 5,
        scratch_shapes=[
            pltpu.VMEM((1, up_rows), f32),
            pltpu.VMEM(up_master.shape, f32),
            pltpu.VMEM(down_master.shape, f32),
            pltpu.VMEM((rows, model), bf16),
            pltpu.VMEM((down_rows, feats), bf16),
            pltpu.VMEM((starts, down_rows, feats), bf16),
            pltpu.VMEM((rows, 1), f32),
            pltpu.VMEM((rows, width), bf16),
            pltpu.VMEM((rows, half), f32),
            pltpu.VMEM((4, rows, half), bf16),
            pltpu.VMEM((2, rows, half), bf16),
            dma((3,)), dma((3,)), dma((1,)), dma((n_tp,)),
            dma((3, lines, UP_CUTS)), dma((lines, UP_CUTS)), dma((lines, UP_CUTS)),
            dma((3, lines, 2)), dma((lines, 2)),
            dma((3, 8, starts, DOWN_CUTS)),
            dma((8, starts, DOWN_CUTS)), dma((8, starts, DOWN_CUTS)),
            dma((2, 2, starts, DOWN_CUTS)), dma((2, starts, DOWN_CUTS)),
            dma((2, starts, 2, DOWN_CUTS)), dma((starts, 2, DOWN_CUTS)),
            dma((4,)), dma((4,)), dma((2,)), dma((2,)), dma((4,)),
        ],
        compiler_params=pltpu.CompilerParams(
            collective_id=0, has_side_effects=True, vmem_limit_bytes=VMEM_LIMIT * MIB
        ),
        cost_estimate=pl.CostEstimate(flops=flops, bytes_accessed=16 * MIB, transcendentals=0),
        name="layer",
    )(tokens, norm_gain[None, :], up_master, down_master)
    return pl.pallas_call(
        finish,
        out_shape=(
            jax.ShapeDtypeStruct((rows, feats), bf16),
            jax.ShapeDtypeStruct((depth, width), bf16),
            jax.ShapeDtypeStruct((width, model), bf16),
        ),
        in_specs=[vmem] * 5,
        out_specs=(hbm,) * 3,
        scratch_shapes=[pltpu.VMEM((rows, feats), bf16), dma((3,))],
        compiler_params=pltpu.CompilerParams(vmem_limit_bytes=8 * MIB),
        name="finish",
    )(*kept)


def solution(mesh):
    n, n_tp = mesh.shape["fs"], mesh.shape["tp"]
    return jax.shard_map(
        functools.partial(fused, n, n_tp),
        mesh=mesh,
        in_specs=(P("fs", "tp"), P("fs"), P("fs", "tp"), P("fs", "tp")),
        out_specs=(P("fs", "tp"), P(None, "tp"), P("tp", None)),
        check_vma=False,
    )
```

```python
import functools

import jax
import jax.numpy as jnp
from jax import lax
from jax.experimental import pallas as pl
from jax.experimental.pallas import tpu as pltpu
from jax.sharding import PartitionSpec as P

UP_CUTS = 2
DOWN_CUTS = 2
COLUMNS = 256
BOTH = 3
LANES = 128
VMEM_LIMIT = 46
MIB = 1024 * 1024


def kernel(
    n, n_tp,
    tokens_hbm, gain_hbm, upm_hbm, downm_hbm,
    up, down, own, take, crossed,
    gain_in, upm_in, downm_in, tok, shard, passing, scale, sums, hidden, kept, give, cross,
    tok_send, tok_recv, gather_send, gather_recv,
    up_send, upz_recv, upy_recv, both_send, both_recv,
    down_send, downz_recv, downy_recv, pass_send, pass_recv, last_send, last_recv,
    pair_send, pair_recv, cross_send, cross_recv, local_sem,
):
    f32, bf16 = jnp.float32, jnp.bfloat16
    f, t = lax.axis_index("fs"), lax.axis_index("tp")
    lines = n // 2
    z, y = f // 2, f % 2
    t1 = t + 1 - 2 * (t % 2)
    t2 = (t + 2) % 4
    t3 = (t1 + 2) % 4
    members = n // n_tp
    starts = members // 2
    owner = f // members
    above, below = (f + 2) % n, (f + n - 2) % n
    across = f + 1 - 2 * y
    has_above, has_below = z < lines - 1, z > 0
    upper, lower = t >= n_tp // 2, t < n_tp // 2
    at_end = jnp.logical_not(has_above & has_below)

    up_rows = upm_in.shape[0]
    down_rows = downm_in.shape[0]
    feats = tokens_hbm.shape[1]
    half = feats // 2
    dcut = down_rows // DOWN_CUTS
    first_cut = max(8, up_rows * BOTH // 128 * 8)
    ucuts = (first_cut, first_cut + (up_rows - first_cut) // 16 * 8, up_rows)

    def remote(src, dst, send, recv, **to):
        return pltpu.make_async_remote_copy(
            src_ref=src, dst_ref=dst, send_sem=send, recv_sem=recv,
            device_id=to, device_id_type=pl.DeviceIdType.MESH,
        )

    def down_block(source, column):
        rows = pl.ds(pl.multiple_of(source % members * down_rows, down_rows), down_rows)
        return down.at[rows, pl.ds(pl.multiple_of(column * feats, feats), feats)]

    loads = [
        pltpu.make_async_copy(upm_hbm, upm_in, local_sem.at[0]),
        pltpu.make_async_copy(gain_hbm, gain_in, local_sem.at[1]),
        pltpu.make_async_copy(downm_hbm, downm_in, local_sem.at[2]),
        pltpu.make_async_copy(
            tokens_hbm, tok.at[:, pl.ds(pl.multiple_of(t * feats, feats), feats)],
            local_sem.at[3],
        ),
    ]
    for load in loads:
        load.start()

    barrier = pltpu.get_barrier_semaphore()
    for other in (t1, t2, t3):
        pl.semaphore_signal(
            barrier, inc=1, device_id={"tp": other}, device_id_type=pl.DeviceIdType.MESH
        )
    pl.semaphore_signal(
        barrier, inc=1, device_id={"fs": across}, device_id_type=pl.DeviceIdType.MESH
    )

    @pl.when(has_above)
    def _():
        pl.semaphore_signal(
            barrier, inc=1, device_id={"fs": above}, device_id_type=pl.DeviceIdType.MESH
        )

    @pl.when(has_below)
    def _():
        pl.semaphore_signal(
            barrier, inc=1, device_id={"fs": below}, device_id_type=pl.DeviceIdType.MESH
        )

    loads[0].wait()
    loads[1].wait()
    gain = jnp.transpose(jnp.broadcast_to(gain_in[...], (LANES, up_rows)))
    for first in range(0, up.shape[1], LANES):
        up[pl.ds(pl.multiple_of(f * up_rows, up_rows), up_rows), pl.ds(first, LANES)] = (
            gain * upm_in[:, pl.ds(first, LANES)]
        ).astype(bf16)

    loads[2].wait()

    @pl.when(owner == t)
    def _():
        down_block(f, t)[...] = downm_in[...].astype(bf16)

    @pl.when(owner == t2)
    def _():
        passing[z % starts] = downm_in[...].astype(bf16)

    @pl.when((owner == t1) | (owner == t3))
    def _():
        shard[...] = downm_in[...].astype(bf16)

    pl.semaphore_wait(
        barrier, 4 + has_above.astype(jnp.int32) + has_below.astype(jnp.int32)
    )

    def up_piece(line, column, u):
        first, last = (ucuts[u], ucuts[u + 1]) if u >= 0 else (0, ucuts[0])
        row = (line * 2 + column) * up_rows + first
        return up.at[pl.ds(pl.multiple_of(row, 8), last - first), :]

    def both_copy(way, line, column, to):
        piece = up_piece(line, column, -1)
        return remote(
            piece, piece, both_send.at[way, line, column], both_recv.at[line, column], fs=to
        )

    def run(copy, start):
        copy.start() if start else copy.wait_send()

    def both_onward(line, column, start):
        @pl.when(has_above & (line <= z))
        def _():
            run(both_copy(0, line, column, above), start)

        @pl.when(has_below & (line >= z))
        def _():
            run(both_copy(1, line, column, below), start)

    def up_copy(way, line, u, to):
        piece = up_piece(line, y, u)
        recv = upy_recv if way == 2 else upz_recv
        return remote(piece, piece, up_send.at[way, line, u], recv.at[line, u], fs=to)

    def up_onward(line, u, start):
        @pl.when(has_above & (line <= z))
        def _():
            run(up_copy(0, line, u, above), start)

        @pl.when(has_below & (line >= z))
        def _():
            run(up_copy(1, line, u, below), start)

        run(up_copy(2, line, u, across), start)

    both_copy(2, z, y, across).start()
    for u in range(UP_CUTS):
        up_onward(z, u, True)
    both_onward(z, y, True)

    def gather_copy(column, to):
        return remote(
            shard, down_block(f, column), gather_send.at[0], gather_recv.at[column], tp=to
        )

    order = ((t3, 0), (t2, 0), (t3, 1), (t2, 1), (t1, 0), (t1, 1), (t, 0), (t, 1))
    passed = (1, 3)
    finals = 7
    early = (0, 1, 2)

    def pass_copies(part, js, q, start, ways=(0, 1)):
        line = t2 * starts + js
        row = ((line * 2 + y) % members) * down_rows + q * dcut
        ci = passed[part]
        here = passing.at[js, pl.ds(q * dcut, dcut), pl.ds(part * half, half)]
        there = down.at[
            pl.ds(pl.multiple_of(row, dcut), dcut),
            pl.ds(pl.multiple_of(t * feats + part * half, half), half),
        ]

        def onward(to):
            return remote(
                here, here, pass_send.at[0, part, js, q], pass_recv.at[part, js, q], fs=to
            )

        if 0 in ways:
            @pl.when(lower & has_below & (line >= z))
            def _():
                run(onward(below), start)

            @pl.when(upper & has_above & (line <= z))
            def _():
                run(onward(above), start)

        if 1 in ways:
            @pl.when((upper & (line <= z)) | (lower & (line >= z)))
            def _():
                over = remote(
                    here, there, pass_send.at[1, part, js, q], downz_recv.at[ci, js, q],
                    tp=t2,
                )
                run(over, start)

    def pass_on(part, q):
        @pl.loop(0, starts)
        def _(js):
            line = t2 * starts + js

            @pl.when((upper & (line < z)) | (lower & (line > z)))
            def _():
                here = passing.at[js, pl.ds(q * dcut, dcut), pl.ds(part * half, half)]
                remote(
                    here, here, pass_send.at[0, part, js, q], pass_recv.at[part, js, q],
                    fs=above,
                ).wait_recv()
                pass_copies(part, js, q, True)

    def pass_start(way):
        @pl.when(owner == t2)
        def _():
            for part in range(2):
                for q in range(DOWN_CUTS):
                    pass_copies(part, z % starts, q, True, (way,))

    @pl.when((owner == t1) | (owner == t3))
    def _():
        gather_copy(t, owner).start()

    pass_start(1)
    loads[3].wait()

    def tok_copy(way, column, to):
        piece = tok.at[:, pl.ds(pl.multiple_of(column * feats, feats), feats)]
        return remote(piece, piece, tok_send.at[way], tok_recv.at[way], tp=to)

    tok_copy(1, t, t2).start()
    tok_copy(0, t, t1).start()

    sums[...] = jnp.zeros(sums.shape, f32)
    both_copy(2, z, 1 - y, across).wait_recv()
    both_onward(z, 1 - y, True)

    def both_relay(line, column):
        @pl.when((line >= 0) & (line < lines))
        def _():
            both_copy(0, line, column, above).wait_recv()
            both_onward(line, column, True)

    def down_piece(ci, js, side, q):
        column, part = order[ci]
        line = t * starts + js
        row = ((line * 2 + side) % members) * down_rows + q * dcut
        return down.at[
            pl.ds(pl.multiple_of(row, dcut), dcut),
            pl.ds(pl.multiple_of(column * feats + part * half, half), half),
        ]

    def down_copy(way, ci, js, q, to):
        piece = down_piece(ci, js, y, q)
        recv = downy_recv if way == 2 else downz_recv
        return remote(
            piece, piece, down_send.at[way, ci, js, q], recv.at[ci, js, q], fs=to
        )

    def down_lines(ci, js, q, start):
        line = t * starts + js
        rising = has_above & (line <= z)
        falling = has_below & (line >= z)
        if ci in passed:
            rising = rising & upper
            falling = falling & lower
        elif start:
            rising = rising & (upper | (line < z))
            falling = falling & (lower | (line > z))

        @pl.when(rising)
        def _():
            run(down_copy(0, ci, js, q, above), start)

        @pl.when(falling)
        def _():
            run(down_copy(1, ci, js, q, below), start)

    def down_over(ci, js, q, start):
        line = t * starts + js
        if ci == finals:
            @pl.when(line == z)
            def _():
                run(down_copy(2, ci, js, q, across), start)
        elif start and ci in early:
            @pl.when(line != z)
            def _():
                down_copy(2, ci, js, q, across).start()
        else:
            run(down_copy(2, ci, js, q, across), start)

    def far_start():
        js = z % starts

        def send(make):
            @pl.when(lower & has_above)
            def _():
                make(0, above).start()

            @pl.when(upper & has_below)
            def _():
                make(1, below).start()

        @pl.when(owner == t)
        def _():
            for ci in (0, 2, 4, 5, 6):
                for q in range(DOWN_CUTS):
                    send(lambda way, to: down_copy(way, ci, js, q, to))
            for q in range(DOWN_CUTS):
                send(lambda way, to: last_copy(way, js, y, q, to))

    def last_copy(way, js, side, q, to):
        piece = down_piece(finals, js, side, q)
        return remote(
            piece, piece, last_send.at[way, js, side, q], last_recv.at[js, side, q], fs=to
        )

    def last_onward(js, side, q, start, sent=False):
        line = t * starts + js
        rising = has_above & (line <= z)
        falling = has_below & (line >= z)
        if sent:
            rising = rising & (upper | (line < z))
            falling = falling & (lower | (line > z))

        @pl.when(rising)
        def _():
            run(last_copy(0, js, side, q, above), start)

        @pl.when(falling)
        def _():
            run(last_copy(1, js, side, q, below), start)

    def relay(ci, q, ways=(0, 1)):
        @pl.loop(0, starts)
        def _(js):
            if 0 in ways:
                if ci in passed and ci not in early:
                    down_copy(0, ci, js, q, above).wait_recv()
                else:
                    @pl.when(t * starts + js != z)
                    def _():
                        down_copy(0, ci, js, q, above).wait_recv()

                down_lines(ci, js, q, True)
            if 1 in ways:
                down_over(ci, js, q, True)

    def relay_line(ci, q):
        relay(ci, q, (0,))

    def relay_over(ci, q):
        relay(ci, q, (1,))

    def last_turn():
        @pl.when(owner == t)
        def _():
            js = z % starts
            for q in range(DOWN_CUTS):
                piece = down_piece(finals, js, 1 - y, q)
                remote(
                    piece, piece, down_send.at[2, finals, js, q],
                    downy_recv.at[finals, js, q], fs=across,
                ).wait_recv()
                last_onward(js, 1 - y, q, True)
                last_onward(js, y, q, True, True)

    def last_relay(side, q):
        @pl.loop(0, starts)
        def _(js):
            @pl.when(t * starts + js != z)
            def _():
                last_copy(0, js, side, q, above).wait_recv()
                last_onward(js, side, q, True, True)

    def relayed(ci):
        @pl.loop(0, starts)
        def _(js):
            for q in range(DOWN_CUTS):
                piece = down_piece(ci, js, 1 - y, q)
                remote(
                    piece, piece, down_send.at[2, ci, js, q], downy_recv.at[ci, js, q],
                    fs=across,
                ).wait_recv()

    @pl.when(owner == t)
    def _():
        for ci in (4, 0):
            gather_copy(order[ci][0], t).wait_recv()

    @pl.when(at_end)
    def _():
        pass_start(0)
        far_start()

    rows_all, width = tok.shape[0], up.shape[1]
    step = min(rows_all, 128)
    low = (z < lines // 2).astype(jnp.int32)
    final = low * (n_tp - 1)

    inside = has_above & has_below
    near = (lower & (z < lines // 2)) | (upper & (z >= lines // 2))
    far = jnp.logical_not(near)

    def share():
        tok_copy(1, t2, t2).wait_recv()
        tok_copy(2, t2, t1).start()

    def scales():
        @pl.loop(0, rows_all // step)
        def _(i):
            rows = pl.ds(pl.multiple_of(i * step, step), step)
            values = tok[rows, :].astype(f32)
            mean_square = jnp.mean(values * values, axis=-1, keepdims=True)
            scale[rows, :] = lax.rsqrt(mean_square + 1e-06)

    def ordered(c):
        return low * c + (1 - low) * (n_tp - 1 - c)

    def reach(c):
        return ordered(c) * starts + starts - 1

    def arrived(c):
        @pl.loop(0, starts)
        def _(js):
            line = c * starts + js
            for u in range(UP_CUTS):
                piece = up_piece(line, 1 - y, u)
                remote(
                    piece, piece, up_send.at[2, line, u], upy_recv.at[line, u], fs=across
                ).wait_recv()

    def before(c, columns):
        part = pl.ds(pl.multiple_of(c * feats, feats), feats)
        return jnp.dot(tok[:, part], up[part, columns], preferred_element_type=f32)

    def accumulate(c):
        arrived(c)

        @pl.loop(0, width // COLUMNS)
        def _(i):
            columns = pl.ds(pl.multiple_of(i * COLUMNS, COLUMNS), COLUMNS)
            sums[:, columns] += before(c, columns)

    def second():
        @pl.loop(0, n_tp)
        def _(c):
            @pl.when(reach(c) == lines - 2)
            def _():
                accumulate(c)

    @pl.loop(1, lines)
    def _(d):
        last = at_end & (d == lines - 1)

        def reached(c, step_c):
            @pl.loop(0, 2)
            def _(j):
                @pl.when(reach(c + j * step_c) <= lines - 3)
                def _():
                    accumulate(c + j * step_c)

        @pl.when(last)
        def _():
            tok_copy(0, t1, t1).wait_recv()
            reached(t, t1 - t)

        @pl.when(last & far)
        def _():
            share()
            tok_copy(2, t3, t1).wait_recv()
            reached(t2, t3 - t2)

        for u in range(UP_CUTS):
            @pl.when(z - d >= 0)
            def _():
                up_copy(0, z - d, u, above).wait_recv()
                up_onward(z - d, u, True)

            @pl.when(z + d < lines)
            def _():
                up_copy(1, z + d, u, below).wait_recv()
                up_onward(z + d, u, True)

            if u == 0:
                @pl.when(last & far)
                def _():
                    second()
                    scales()

                pl.when(last & near)(share)

        for column in (y, 1 - y):
            both_relay(z - d, column)
            both_relay(z + d, column)

        for k in range(len(early)):
            @pl.when((owner == t) & (d == k + 1))
            def _():
                for q in range(DOWN_CUTS):
                    if early[k] in passed:
                        down_copy(0, early[k], z % starts, q, above).wait_recv()
                    down_copy(2, early[k], z % starts, q, across).start()

    @pl.when(has_above & has_below)
    def _():
        pass_start(0)
        far_start()

    def when(condition, *moves):
        @pl.when(condition)
        def _():
            for move, which, cuts in moves:
                for q in cuts:
                    move(which, q)

    every = range(DOWN_CUTS)
    @pl.when(owner == t)
    def _():
        for q in every:
            down_over(finals, z % starts, q, True)

    def all_tokens():
        tok_copy(0, t1, t1).wait_recv()
        tok_copy(2, t3, t1).wait_recv()

    when(inside & near & (owner != t), (relay_line, 0, every), (relay_line, 2, every))
    when(inside, (pass_on, 0, every))
    when(inside & far, (pass_on, 1, every))
    pl.when(inside)(share)
    when(inside & near & (owner == t), (relay_line, 0, every))
    when(inside & near, (relay_over, 0, every), (relay, 1, every))
    pl.when(inside)(all_tokens)
    for c in range(n_tp - 1):
        @pl.when(inside)
        def _():
            accumulate(ordered(c))

        when(inside & near, (pass_on, 1, every[c :: n_tp - 1]))
    when(inside & near & (owner == t), (relay_line, 2, every))
    when(inside & near, (relay_over, 2, every), (relay, 3, every))
    when(inside & near, *((relay_line, ci, every) for ci in (4, 5, 6)))
    pl.when(inside)(scales)
    when(inside & far, (relay, 0, every))
    when(at_end & far, (relay, 0, every[:1]))
    when(at_end & near, (pass_on, 0, every[:1]))
    @pl.when(at_end & near)
    def _():
        tok_copy(2, t3, t1).wait_recv()
        second()
        scales()

    arrived(final)
    tiles = width // COLUMNS
    steps = 4
    for k in range(steps):
        @pl.loop(k * tiles // steps, (k + 1) * tiles // steps)
        def _(i):
            columns = pl.ds(pl.multiple_of(i * COLUMNS, COLUMNS), COLUMNS)
            value = jnp.maximum((sums[:, columns] + before(final, columns)) * scale[...], 0.0)
            hidden[:, columns] = (value * value).astype(bf16)

        if k == 0:
            when(inside & far, (relay, 2, every[:1]))
            when(at_end & near, (pass_on, 0, every[1:]))
            when(at_end & far, (relay, 0, every[1:]))
        if k == 1:
            when(inside & far, (relay, 2, every[1:]))
            when(at_end & near, (relay, 0, every[:1]))
            when(at_end & far, (relay, 1, every[:1]))
        if k == 2:
            when(inside & far, (relay_line, 4, every[:1]))
            when(at_end & near, (relay, 0, every[1:]))
            when(at_end & far, (relay, 2, every[:1]))

    when(at_end & far, (relay, 1, every[1:]), (relay, 2, every[1:]))
    when(inside & far, (relay_line, 4, every[1:]))
    when((at_end & near) | (inside & far), (relay, 1, every))
    pl.when(at_end)(last_turn)

    def product(ci):
        column, part = order[ci]
        first = pl.multiple_of(column * feats + part * half, half)
        return jnp.dot(hidden[...], down[:, pl.ds(first, half)], preferred_element_type=f32)

    def pair_copy(i):
        return remote(give.at[i], take.at[i], pair_send.at[i], pair_recv.at[i], tp=t1)

    def cross_copy(i):
        return remote(
            cross.at[i], crossed.at[i], cross_send.at[i], cross_recv.at[i], tp=t2
        )

    def cross_over(i):
        pair_copy(i).wait_recv()

        @pl.loop(0, rows_all // step)
        def _(j):
            rows = pl.ds(pl.multiple_of(j * step, step), step)
            cross[i, rows, :] = (kept[rows, :] + take[i, rows, :].astype(f32)).astype(bf16)

        cross_copy(i).start()

    def forward(ci):
        when(at_end, (relay_line, ci, every))
        for q in every:
            relay_over(ci, q)

    def drain_up():
        @pl.loop(0, lines)
        def _(line):
            for u in range(UP_CUTS):
                up_onward(line, u, False)
            for column in range(2):
                both_onward(line, column, False)

        both_copy(2, z, y, across).wait_send()

        @pl.loop(0, starts)
        def _(js):
            for q in range(DOWN_CUTS):
                for part in range(2):
                    pass_copies(part, js, q, False)

        @pl.when((owner == t1) | (owner == t3))
        def _():
            gather_copy(t, owner).wait_send()

        tok_copy(0, t, t1).wait_send()
        tok_copy(1, t, t2).wait_send()
        tok_copy(2, t2, t1).wait_send()

    def drain_down(which):
        @pl.loop(0, starts)
        def _(js):
            for q in range(DOWN_CUTS):
                for ci in which:
                    if ci != finals:
                        down_lines(ci, js, q, False)
                    else:
                        for side in range(2):
                            last_onward(js, side, q, False)
                    down_over(ci, js, q, False)

    relayed(0)
    give[0] = product(0).astype(bf16)
    pair_copy(0).start()
    when(inside & far, (relay_line, 5, every))
    when(at_end & near, (pass_on, 1, every))
    relayed(1)
    kept[...] = product(1)
    when(inside & far, (relay_line, 6, every), (last_relay, y, every))
    when(inside & near, *((last_relay, side, every) for side in (y, 1 - y)))
    when(at_end & near, (relay, 2, every))
    when(at_end & far, (pass_on, 0, every), (pass_on, 1, every))
    when(at_end | far, (relay, 3, every))
    cross_over(0)
    relayed(2)
    give[1] = product(2).astype(bf16)
    pair_copy(1).start()
    forward(4)
    pl.when(inside)(last_turn)
    when(inside & far, (last_relay, 1 - y, every))
    relayed(3)
    kept[...] = product(3)
    cross_over(1)
    forward(5)
    forward(6)
    relayed(4)
    give[2] = product(4).astype(bf16)
    pair_copy(2).start()
    when(at_end, (last_relay, y, (0,)))
    when(at_end, (last_relay, 1 - y, (0,)))
    relayed(5)
    give[3] = product(5).astype(bf16)
    pair_copy(3).start()
    when(at_end, (last_relay, y, (1,)))
    when(at_end, (last_relay, 1 - y, (1,)))
    drain_up()
    drain_down(range(6))
    own[1] = product(7)
    relayed(6)
    own[0] = product(6)
    for i in range(2):
        pair_copy(2 + i).wait_recv()
        cross_copy(i).wait_recv()

    drain_down(range(6, 8))
    for i in range(4):
        pair_copy(i).wait_send()
    for i in range(2):
        cross_copy(i).wait_send()


def finish(up, down, own, take, crossed, mixed_hbm, up_hbm, down_hbm, mixed, sems):
    copies = [
        pltpu.make_async_copy(up, up_hbm, sems.at[0]),
        pltpu.make_async_copy(down, down_hbm, sems.at[1]),
    ]
    for copy in copies:
        copy.start()
    rows_all, half = own.shape[1:]
    step = min(rows_all, 128)
    for i in range(2):
        @pl.loop(0, rows_all // step)
        def _(j):
            rows = pl.ds(pl.multiple_of(j * step, step), step)
            mixed[rows, pl.ds(i * half, half)] = (
                own[i, rows, :] + take[2 + i, rows, :].astype(jnp.float32)
                + crossed[i, rows, :].astype(jnp.float32)
            ).astype(mixed.dtype)

    copies.append(pltpu.make_async_copy(mixed, mixed_hbm, sems.at[2]))
    copies[2].start()
    for copy in copies:
        copy.wait()


def fused(n, n_tp, tokens, norm_gain, up_master, down_master):
    rows, feats = tokens.shape
    up_rows, width = up_master.shape
    down_rows = down_master.shape[0]
    depth = up_rows * n
    model = feats * n_tp
    half = feats // 2
    lines, starts = n // 2, n // n_tp // 2
    bf16, f32 = jnp.bfloat16, jnp.float32
    dma = pltpu.SemaphoreType.DMA
    vmem = pl.BlockSpec(memory_space=pltpu.VMEM)
    hbm = pl.BlockSpec(memory_space=pltpu.HBM)
    flops = 4 * rows * depth * width
    kept = pl.pallas_call(
        functools.partial(kernel, n, n_tp),
        out_shape=(
            pltpu.VMEM((depth, width), bf16),
            pltpu.VMEM((width, model), bf16),
            pltpu.VMEM((2, rows, half), f32),
            pltpu.VMEM((4, rows, half), bf16),
            pltpu.VMEM((2, rows, half), bf16),
        ),
        in_specs=[hbm] * 4,
        out_specs=(vmem,) * 5,
        scratch_shapes=[
            pltpu.VMEM((1, up_rows), f32),
            pltpu.VMEM(up_master.shape, f32),
            pltpu.VMEM(down_master.shape, f32),
            pltpu.VMEM((rows, model), bf16),
            pltpu.VMEM((down_rows, feats), bf16),
            pltpu.VMEM((starts, down_rows, feats), bf16),
            pltpu.VMEM((rows, 1), f32),
            pltpu.VMEM((rows, width), f32),
            pltpu.VMEM((rows, width), bf16),
            pltpu.VMEM((rows, half), f32),
            pltpu.VMEM((4, rows, half), bf16),
            pltpu.VMEM((2, rows, half), bf16),
            dma((3,)), dma((3,)), dma((1,)), dma((n_tp,)),
            dma((3, lines, UP_CUTS)), dma((lines, UP_CUTS)), dma((lines, UP_CUTS)),
            dma((3, lines, 2)), dma((lines, 2)),
            dma((3, 8, starts, DOWN_CUTS)),
            dma((8, starts, DOWN_CUTS)), dma((8, starts, DOWN_CUTS)),
            dma((2, 2, starts, DOWN_CUTS)), dma((2, starts, DOWN_CUTS)),
            dma((2, starts, 2, DOWN_CUTS)), dma((starts, 2, DOWN_CUTS)),
            dma((4,)), dma((4,)), dma((2,)), dma((2,)), dma((4,)),
        ],
        compiler_params=pltpu.CompilerParams(
            collective_id=0, has_side_effects=True, vmem_limit_bytes=VMEM_LIMIT * MIB
        ),
        cost_estimate=pl.CostEstimate(flops=flops, bytes_accessed=16 * MIB, transcendentals=0),
        name="layer",
    )(tokens, norm_gain[None, :], up_master, down_master)
    return pl.pallas_call(
        finish,
        out_shape=(
            jax.ShapeDtypeStruct((rows, feats), bf16),
            jax.ShapeDtypeStruct((depth, width), bf16),
            jax.ShapeDtypeStruct((width, model), bf16),
        ),
        in_specs=[vmem] * 5,
        out_specs=(hbm,) * 3,
        scratch_shapes=[pltpu.VMEM((rows, feats), bf16), dma((3,))],
        compiler_params=pltpu.CompilerParams(vmem_limit_bytes=8 * MIB),
        name="finish",
    )(*kept)


def solution(mesh):
    n, n_tp = mesh.shape["fs"], mesh.shape["tp"]
    return jax.shard_map(
        functools.partial(fused, n, n_tp),
        mesh=mesh,
        in_specs=(P("fs", "tp"), P("fs"), P("fs", "tp"), P("fs", "tp")),
        out_specs=(P("fs", "tp"), P(None, "tp"), P("tp", None)),
        check_vma=False,
    )
```

```python
import functools

import jax
import jax.numpy as jnp
from jax import lax
from jax.experimental import pallas as pl
from jax.experimental.pallas import tpu as pltpu
from jax.sharding import PartitionSpec as P

UP_CUTS = 2
DOWN_CUTS = 2
COLUMNS = 256
BOTH = 3
LANES = 128
VMEM_LIMIT = 46
MIB = 1024 * 1024


def kernel(
    n, n_tp,
    tokens_hbm, gain_hbm, upm_hbm, downm_hbm,
    up, down, own, take, crossed,
    gain_in, upm_in, downm_in, tok, shard, passing, scale, sums, hidden, kept, give, cross,
    tok_recv, gather_recv, up_send, upz_recv, upy_recv, both_recv,
    down_send, downz_recv, downy_recv, pass_send, pass_recv, last_recv,
    pair_recv, cross_recv, once_send, local_sem,
):
    f32, bf16 = jnp.float32, jnp.bfloat16
    f, t = lax.axis_index("fs"), lax.axis_index("tp")
    lines = n // 2
    z, y = f // 2, f % 2
    t1 = t + 1 - 2 * (t % 2)
    t2 = (t + 2) % 4
    t3 = (t1 + 2) % 4
    members = n // n_tp
    starts = members // 2
    owner = f // members
    above, below = (f + 2) % n, (f + n - 2) % n
    across = f + 1 - 2 * y
    has_above, has_below = z < lines - 1, z > 0
    upper, lower = t >= n_tp // 2, t < n_tp // 2
    at_end = jnp.logical_not(has_above & has_below)

    up_rows = upm_in.shape[0]
    down_rows = downm_in.shape[0]
    rows_all, feats = tokens_hbm.shape
    half = feats // 2
    width = up.shape[1]
    (up_over, down_over_send, last_over, gather_send, tok_send, pair_send, cross_send) = (
        once_send.at[i] for i in range(7)
    )
    dcut = down_rows // DOWN_CUTS
    first_cut = max(8, up_rows * BOTH // 128 * 8)
    ucuts = (first_cut, first_cut + (up_rows - first_cut) // 16 * 8, up_rows)

    def remote(src, dst, send, recv, **to):
        return pltpu.make_async_remote_copy(
            src_ref=src, dst_ref=dst, send_sem=send, recv_sem=recv,
            device_id=to, device_id_type=pl.DeviceIdType.MESH,
        )

    def down_block(source, column):
        rows = pl.ds(pl.multiple_of(source % members * down_rows, down_rows), down_rows)
        return down.at[rows, pl.ds(pl.multiple_of(column * feats, feats), feats)]

    loads = [
        pltpu.make_async_copy(upm_hbm, upm_in, local_sem.at[0]),
        pltpu.make_async_copy(gain_hbm, gain_in, local_sem.at[1]),
        pltpu.make_async_copy(downm_hbm, downm_in, local_sem.at[2]),
        pltpu.make_async_copy(
            tokens_hbm, tok.at[:, pl.ds(pl.multiple_of(t * feats, feats), feats)],
            local_sem.at[3],
        ),
    ]
    for load in loads:
        load.start()

    barrier = pltpu.get_barrier_semaphore()
    for other in (t1, t2, t3):
        pl.semaphore_signal(
            barrier, inc=1, device_id={"tp": other}, device_id_type=pl.DeviceIdType.MESH
        )
    pl.semaphore_signal(
        barrier, inc=1, device_id={"fs": across}, device_id_type=pl.DeviceIdType.MESH
    )

    @pl.when(has_above)
    def _():
        pl.semaphore_signal(
            barrier, inc=1, device_id={"fs": above}, device_id_type=pl.DeviceIdType.MESH
        )

    @pl.when(has_below)
    def _():
        pl.semaphore_signal(
            barrier, inc=1, device_id={"fs": below}, device_id_type=pl.DeviceIdType.MESH
        )

    loads[0].wait()
    loads[1].wait()
    gain = jnp.transpose(jnp.broadcast_to(gain_in[...], (LANES, up_rows)))
    for first in range(0, up.shape[1], LANES):
        up[pl.ds(pl.multiple_of(f * up_rows, up_rows), up_rows), pl.ds(first, LANES)] = (
            gain * upm_in[:, pl.ds(first, LANES)]
        ).astype(bf16)

    loads[2].wait()

    @pl.when(owner == t)
    def _():
        down_block(f, t)[...] = downm_in[...].astype(bf16)

    @pl.when(owner == t2)
    def _():
        passing[z % starts] = downm_in[...].astype(bf16)

    @pl.when((owner == t1) | (owner == t3))
    def _():
        shard[...] = downm_in[...].astype(bf16)

    pl.semaphore_wait(
        barrier, 4 + has_above.astype(jnp.int32) + has_below.astype(jnp.int32)
    )

    def up_piece(line, column, u):
        first, last = (ucuts[u], ucuts[u + 1]) if u >= 0 else (0, ucuts[0])
        row = (line * 2 + column) * up_rows + first
        return up.at[pl.ds(pl.multiple_of(row, 8), last - first), :]

    def both_copy(way, line, column, to):
        piece = up_piece(line, column, -1)
        return remote(
            piece, piece, up_over if way == 2 else up_send.at[way, line],
            both_recv.at[line, column], fs=to,
        )

    def spent(ref, send):
        remote(ref, ref, send, local_sem.at[0], fs=across).wait_send()

    def landed(ref, recv):
        remote(ref, ref, local_sem.at[0], recv, fs=across).wait_recv()

    def both_onward(line, column):
        @pl.when(has_above & (line <= z))
        def _():
            both_copy(0, line, column, above).start()

        @pl.when(has_below & (line >= z))
        def _():
            both_copy(1, line, column, below).start()

    def up_copy(way, line, u, to):
        piece = up_piece(line, y, u)
        if way == 2:
            return remote(piece, piece, up_over, upy_recv.at[line // starts], fs=to)
        return remote(piece, piece, up_send.at[way, line], upz_recv.at[line, u], fs=to)

    def up_onward(line, u):
        @pl.when(has_above & (line <= z))
        def _():
            up_copy(0, line, u, above).start()

        @pl.when(has_below & (line >= z))
        def _():
            up_copy(1, line, u, below).start()

        up_copy(2, line, u, across).start()

    both_copy(2, z, y, across).start()
    for u in range(UP_CUTS):
        up_onward(z, u)
    both_onward(z, y)

    def gather_copy(column, to):
        return remote(
            shard, down_block(f, column), gather_send, gather_recv.at[column], tp=to
        )

    order = ((t3, 0), (t2, 0), (t3, 1), (t2, 1), (t1, 0), (t1, 1), (t, 0), (t, 1))
    passed = (1, 3)
    finals = 7
    early = (0, 1, 2)

    passes_down = lower & has_below
    passes_up = upper & has_above

    def pass_copies(part, js, q, ways=(0, 1)):
        line = t2 * starts + js
        row = ((line * 2 + y) % members) * down_rows + q * dcut
        here = passing.at[js, pl.ds(q * dcut, dcut), pl.ds(part * half, half)]
        there = down.at[
            pl.ds(pl.multiple_of(row, dcut), dcut),
            pl.ds(pl.multiple_of(t * feats + part * half, half), half),
        ]

        def onward(to):
            remote(here, here, pass_send.at[0, js], pass_recv.at[part, js, q], fs=to).start()

        if 0 in ways:
            @pl.when(passes_down & (line >= z))
            def _():
                onward(below)

            @pl.when(passes_up & (line <= z))
            def _():
                onward(above)

        if 1 in ways:
            @pl.when((upper & (line <= z)) | (lower & (line >= z)))
            def _():
                remote(
                    here, there, pass_send.at[1, js], downz_recv.at[passed[part], js, q],
                    tp=t2,
                ).start()

    def pass_on(part, q):
        @pl.loop(0, starts)
        def _(js):
            line = t2 * starts + js

            @pl.when((upper & (line < z)) | (lower & (line > z)))
            def _():
                here = passing.at[js, pl.ds(q * dcut, dcut), pl.ds(part * half, half)]
                landed(here, pass_recv.at[part, js, q])
                pass_copies(part, js, q)

    def pass_start(way):
        @pl.when(owner == t2)
        def _():
            for part in range(2):
                for q in range(DOWN_CUTS):
                    pass_copies(part, z % starts, q, (way,))

    @pl.when((owner == t1) | (owner == t3))
    def _():
        gather_copy(t, owner).start()

    pass_start(1)
    loads[3].wait()

    def tok_copy(way, column, to):
        piece = tok.at[:, pl.ds(pl.multiple_of(column * feats, feats), feats)]
        return remote(piece, piece, tok_send, tok_recv.at[way], tp=to)

    tok_copy(1, t, t2).start()
    tok_copy(0, t, t1).start()

    sums[...] = jnp.zeros(sums.shape, f32)
    both_copy(2, z, 1 - y, across).wait_recv()
    both_onward(z, 1 - y)

    def both_relay(line, column):
        @pl.when((line >= 0) & (line < lines))
        def _():
            both_copy(0, line, column, above).wait_recv()
            both_onward(line, column)

    def down_piece(ci, js, side, q):
        column, part = order[ci]
        line = t * starts + js
        row = ((line * 2 + side) % members) * down_rows + q * dcut
        return down.at[
            pl.ds(pl.multiple_of(row, dcut), dcut),
            pl.ds(pl.multiple_of(column * feats + part * half, half), half),
        ]

    def down_copy(way, ci, js, q, to):
        piece = down_piece(ci, js, y, q)
        if way == 2:
            send = last_over if ci == finals else down_over_send
            return remote(piece, piece, send, downy_recv.at[ci], fs=to)
        return remote(piece, piece, down_send.at[way, js], downz_recv.at[ci, js, q], fs=to)

    def down_lines(ci, js, q):
        line = t * starts + js
        rising = has_above & (line <= z)
        falling = has_below & (line >= z)
        if ci in passed:
            rising = rising & upper
            falling = falling & lower
        else:
            rising = rising & (upper | (line < z))
            falling = falling & (lower | (line > z))

        @pl.when(rising)
        def _():
            down_copy(0, ci, js, q, above).start()

        @pl.when(falling)
        def _():
            down_copy(1, ci, js, q, below).start()

    def down_over(ci, js, q):
        if ci in early:
            @pl.when(t * starts + js != z)
            def _():
                down_copy(2, ci, js, q, across).start()
        else:
            down_copy(2, ci, js, q, across).start()

    def far_start():
        js = z % starts

        def send(make):
            @pl.when(lower & has_above)
            def _():
                make(0, above).start()

            @pl.when(upper & has_below)
            def _():
                make(1, below).start()

        @pl.when(owner == t)
        def _():
            for ci in (0, 2, 4, 5, 6):
                for q in range(DOWN_CUTS):
                    send(lambda way, to: down_copy(way, ci, js, q, to))
            for q in range(DOWN_CUTS):
                send(lambda way, to: last_copy(way, js, y, q, to))

    def last_copy(way, js, side, q, to):
        piece = down_piece(finals, js, side, q)
        return remote(
            piece, piece, down_send.at[way, js], last_recv.at[js, side, q], fs=to
        )

    def last_onward(js, side, q, sent=True):
        line = t * starts + js
        rising = has_above & (line <= z)
        falling = has_below & (line >= z)
        if sent:
            rising = rising & (upper | (line < z))
            falling = falling & (lower | (line > z))

        @pl.when(rising)
        def _():
            last_copy(0, js, side, q, above).start()

        @pl.when(falling)
        def _():
            last_copy(1, js, side, q, below).start()

    def relay(ci, q, ways=(0, 1)):
        @pl.loop(0, starts)
        def _(js):
            if 0 in ways:
                if ci in passed and ci not in early:
                    down_copy(0, ci, js, q, above).wait_recv()
                else:
                    @pl.when(t * starts + js != z)
                    def _():
                        down_copy(0, ci, js, q, above).wait_recv()

                down_lines(ci, js, q)
            if 1 in ways:
                down_over(ci, js, q)

    def relay_line(ci, q):
        relay(ci, q, (0,))

    def relay_over(ci, q):
        relay(ci, q, (1,))

    def last_turn():
        @pl.when(owner == t)
        def _():
            js = z % starts
            landed(down.at[pl.ds(0, down_rows), pl.ds(0, half)], downy_recv.at[finals])
            for q in range(DOWN_CUTS):
                last_onward(js, 1 - y, q, False)
                last_onward(js, y, q)

    def last_relay(side, q):
        @pl.loop(0, starts)
        def _(js):
            @pl.when(t * starts + js != z)
            def _():
                last_copy(0, js, side, q, above).wait_recv()
                last_onward(js, side, q)

    def relayed(ci):
        landed(down.at[pl.ds(0, starts * down_rows), pl.ds(0, half)], downy_recv.at[ci])

    @pl.when(owner == t)
    def _():
        for ci in (4, 0):
            gather_copy(order[ci][0], t).wait_recv()

    @pl.when(at_end)
    def _():
        pass_start(0)
        far_start()

    step = min(rows_all, 128)
    low = (z < lines // 2).astype(jnp.int32)
    final = low * (n_tp - 1)

    inside = has_above & has_below
    near = (lower & (z < lines // 2)) | (upper & (z >= lines // 2))
    far = jnp.logical_not(near)

    def share():
        tok_copy(1, t2, t2).wait_recv()
        tok_copy(2, t2, t1).start()

    def scales():
        @pl.loop(0, rows_all // step)
        def _(i):
            rows = pl.ds(pl.multiple_of(i * step, step), step)
            values = tok[rows, :].astype(f32)
            mean_square = jnp.mean(values * values, axis=-1, keepdims=True)
            scale[rows, :] = lax.rsqrt(mean_square + 1e-06)

    def ordered(c):
        return low * c + (1 - low) * (n_tp - 1 - c)

    def reach(c):
        return ordered(c) * starts + starts - 1

    rest = up_rows - first_cut

    def arrived(c):
        landed(up.at[pl.ds(0, starts * rest), :], upy_recv.at[c])

    def before(c, columns):
        part = pl.ds(pl.multiple_of(c * feats, feats), feats)
        return jnp.dot(tok[:, part], up[part, columns], preferred_element_type=f32)

    def accumulate(c):
        arrived(c)

        @pl.loop(0, width // COLUMNS)
        def _(i):
            columns = pl.ds(pl.multiple_of(i * COLUMNS, COLUMNS), COLUMNS)
            sums[:, columns] += before(c, columns)

    def second():
        @pl.loop(0, n_tp)
        def _(c):
            @pl.when(reach(c) == lines - 2)
            def _():
                accumulate(c)

    @pl.loop(1, lines)
    def _(d):
        last = at_end & (d == lines - 1)

        def reached(c, step_c):
            @pl.loop(0, 2)
            def _(j):
                @pl.when(reach(c + j * step_c) <= lines - 3)
                def _():
                    accumulate(c + j * step_c)

        @pl.when(last)
        def _():
            tok_copy(0, t1, t1).wait_recv()
            reached(t, t1 - t)

        @pl.when(last & far)
        def _():
            share()
            tok_copy(2, t3, t1).wait_recv()
            reached(t2, t3 - t2)

        for u in range(UP_CUTS):
            @pl.when(z - d >= 0)
            def _():
                up_copy(0, z - d, u, above).wait_recv()
                up_onward(z - d, u)

            @pl.when(z + d < lines)
            def _():
                up_copy(1, z + d, u, below).wait_recv()
                up_onward(z + d, u)

            if u == 0:
                @pl.when(last & far)
                def _():
                    second()
                    scales()

                pl.when(last & near)(share)

        for column in (y, 1 - y):
            both_relay(z - d, column)
            both_relay(z + d, column)

        for k in range(len(early)):
            @pl.when((owner == t) & (d == k + 1))
            def _():
                for q in range(DOWN_CUTS):
                    if early[k] in passed:
                        down_copy(0, early[k], z % starts, q, above).wait_recv()
                    down_copy(2, early[k], z % starts, q, across).start()

    @pl.when(has_above & has_below)
    def _():
        pass_start(0)
        far_start()

    def when(condition, *moves):
        @pl.when(condition)
        def _():
            for move, which, cuts in moves:
                for q in cuts:
                    move(which, q)

    every = range(DOWN_CUTS)
    @pl.when(owner == t)
    def _():
        for q in every:
            down_copy(2, finals, z % starts, q, across).start()

    def all_tokens():
        tok_copy(0, t1, t1).wait_recv()
        tok_copy(2, t3, t1).wait_recv()

    when(inside & near & (owner != t), (relay_line, 0, every), (relay_line, 2, every))
    when(inside, (pass_on, 0, every))
    when(inside & far, (pass_on, 1, every))
    pl.when(inside)(share)
    when(inside & near & (owner == t), (relay_line, 0, every))
    when(inside & near, (relay_over, 0, every), (relay, 1, every))
    pl.when(inside)(all_tokens)
    for c in range(n_tp - 1):
        @pl.when(inside)
        def _():
            accumulate(ordered(c))

        when(inside & near, (pass_on, 1, every[c :: n_tp - 1]))
    when(inside & near & (owner == t), (relay_line, 2, every))
    when(inside & near, (relay_over, 2, every), (relay, 3, every))
    when(inside & near, *((relay_line, ci, every) for ci in (4, 5, 6)))
    pl.when(inside)(scales)
    when(inside & far, (relay, 0, every))
    when(at_end & far, (relay, 0, every[:1]))
    when(at_end & near, (pass_on, 0, every[:1]))
    @pl.when(at_end & near)
    def _():
        tok_copy(2, t3, t1).wait_recv()
        second()
        scales()

    arrived(final)
    tiles = width // COLUMNS
    steps = 4
    for k in range(steps):
        @pl.loop(k * tiles // steps, (k + 1) * tiles // steps)
        def _(i):
            columns = pl.ds(pl.multiple_of(i * COLUMNS, COLUMNS), COLUMNS)
            value = jnp.maximum((sums[:, columns] + before(final, columns)) * scale[...], 0.0)
            hidden[:, columns] = (value * value).astype(bf16)

        if k == 0:
            when(inside & far, (relay, 2, every[:1]))
            when(at_end & near, (pass_on, 0, every[1:]))
            when(at_end & far, (relay, 0, every[1:]))
        if k == 1:
            when(inside & far, (relay, 2, every[1:]))
            when(at_end & near, (relay, 0, every[:1]))
            when(at_end & far, (relay, 1, every[:1]))
        if k == 2:
            when(inside & far, (relay_line, 4, every[:1]))
            when(at_end & near, (relay, 0, every[1:]))
            when(at_end & far, (relay, 2, every[:1]))

    when(at_end & far, (relay, 1, every[1:]), (relay, 2, every[1:]))
    when(inside & far, (relay_line, 4, every[1:]))
    when((at_end & near) | (inside & far), (relay, 1, every))
    pl.when(at_end)(last_turn)

    def product(ci):
        column, part = order[ci]
        first = pl.multiple_of(column * feats + part * half, half)
        return jnp.dot(hidden[...], down[:, pl.ds(first, half)], preferred_element_type=f32)

    def pair_copy(i):
        return remote(give.at[i], take.at[i], pair_send, pair_recv.at[i], tp=t1)

    def cross_copy(i):
        return remote(cross.at[i], crossed.at[i], cross_send, cross_recv.at[i], tp=t2)

    def cross_over(i):
        pair_copy(i).wait_recv()

        @pl.loop(0, rows_all // step)
        def _(j):
            rows = pl.ds(pl.multiple_of(j * step, step), step)
            cross[i, rows, :] = (kept[rows, :] + take[i, rows, :].astype(f32)).astype(bf16)

        cross_copy(i).start()

    def forward(ci):
        when(at_end, (relay_line, ci, every))
        for q in every:
            relay_over(ci, q)

    def drain():
        @pl.loop(0, lines)
        def _(line):
            for way, onward in ((0, has_above & (line <= z)), (1, has_below & (line >= z))):
                @pl.when(onward)
                def _():
                    spent(up.at[pl.ds(0, up_rows + first_cut), :], up_send.at[way, line])

        spent(up.at[pl.ds(0, lines * rest + first_cut), :], up_over)

        @pl.loop(0, starts)
        def _(js):
            line = t2 * starts + js

            @pl.when((passes_down & (line >= z)) | (passes_up & (line <= z)))
            def _():
                spent(passing.at[js], pass_send.at[0, js])

            @pl.when((upper & (line <= z)) | (lower & (line >= z)))
            def _():
                spent(passing.at[js], pass_send.at[1, js])

        @pl.when((owner == t1) | (owner == t3))
        def _():
            spent(shard, gather_send)

        spent(tok.at[:, pl.ds(0, 3 * feats)], tok_send)

    def drain_down():
        @pl.loop(0, starts)
        def _(js):
            line = t * starts + js
            for way, onward, most in (
                (0, has_above & (line <= z), upper), (1, has_below & (line >= z), lower),
            ):
                for condition, pieces in ((most, 9), (jnp.logical_not(most), 7)):
                    @pl.when(onward & condition)
                    def _():
                        amount = pieces * down_rows // 8
                        spent(tok.at[pl.ds(0, amount), :], down_send.at[way, js])

        spent(down.at[pl.ds(0, starts * down_rows), pl.ds(0, 7 * half)], down_over_send)

        @pl.when(owner == t)
        def _():
            spent(down.at[pl.ds(0, down_rows), pl.ds(0, half)], last_over)

    relayed(0)
    give[0] = product(0).astype(bf16)
    pair_copy(0).start()
    when(inside & far, (relay_line, 5, every))
    when(at_end & near, (pass_on, 1, every))
    relayed(1)
    kept[...] = product(1)
    when(inside & far, (relay_line, 6, every), (last_relay, y, every))
    when(inside & near, *((last_relay, side, every) for side in (y, 1 - y)))
    when(at_end & near, (relay, 2, every))
    when(at_end & far, (pass_on, 0, every), (pass_on, 1, every))
    when(at_end | far, (relay, 3, every))
    cross_over(0)
    relayed(2)
    give[1] = product(2).astype(bf16)
    pair_copy(1).start()
    forward(4)
    pl.when(inside)(last_turn)
    when(inside & far, (last_relay, 1 - y, every))
    relayed(3)
    kept[...] = product(3)
    cross_over(1)
    forward(5)
    forward(6)
    relayed(4)
    give[2] = product(4).astype(bf16)
    pair_copy(2).start()
    when(at_end, (last_relay, y, (0,)))
    when(at_end, (last_relay, 1 - y, (0,)))
    relayed(5)
    give[3] = product(5).astype(bf16)
    pair_copy(3).start()
    when(at_end, (last_relay, y, (1,)))
    when(at_end, (last_relay, 1 - y, (1,)))
    drain()
    own[1] = product(7)
    if down_rows % LANES == 0:
        def partly(side):
            def term(js):
                part = pl.ds(
                    pl.multiple_of((2 * js + side) * down_rows, down_rows), down_rows
                )
                first = pl.multiple_of(t * feats, feats)
                return jnp.dot(
                    hidden[:, part], down[part, pl.ds(first, half)],
                    preferred_element_type=f32,
                )

            return sum((term(js) for js in range(1, starts)), term(0))

        own[0] = partly(y)
        relayed(6)
        own[0] += partly(1 - y)
    else:
        relayed(6)
        own[0] = product(6)
    for i in range(2):
        pair_copy(2 + i).wait_recv()
        cross_copy(i).wait_recv()

    drain_down()
    spent(give, pair_send)
    spent(cross, cross_send)


def finish(up, down, own, take, crossed, mixed_hbm, up_hbm, down_hbm, mixed, sems):
    copies = [
        pltpu.make_async_copy(up, up_hbm, sems.at[0]),
        pltpu.make_async_copy(down, down_hbm, sems.at[1]),
    ]
    for copy in copies:
        copy.start()
    rows_all, half = own.shape[1:]
    step = min(rows_all, 128)
    for i in range(2):
        @pl.loop(0, rows_all // step)
        def _(j):
            rows = pl.ds(pl.multiple_of(j * step, step), step)
            mixed[rows, pl.ds(i * half, half)] = (
                own[i, rows, :] + take[2 + i, rows, :].astype(jnp.float32)
                + crossed[i, rows, :].astype(jnp.float32)
            ).astype(mixed.dtype)

    copies.append(pltpu.make_async_copy(mixed, mixed_hbm, sems.at[2]))
    copies[2].start()
    for copy in copies:
        copy.wait()


def fused(n, n_tp, tokens, norm_gain, up_master, down_master):
    rows, feats = tokens.shape
    up_rows, width = up_master.shape
    down_rows = down_master.shape[0]
    depth = up_rows * n
    model = feats * n_tp
    half = feats // 2
    lines, starts = n // 2, n // n_tp // 2
    bf16, f32 = jnp.bfloat16, jnp.float32
    dma = pltpu.SemaphoreType.DMA
    vmem = pl.BlockSpec(memory_space=pltpu.VMEM)
    hbm = pl.BlockSpec(memory_space=pltpu.HBM)
    flops = 4 * rows * depth * width
    kept = pl.pallas_call(
        functools.partial(kernel, n, n_tp),
        out_shape=(
            pltpu.VMEM((depth, width), bf16),
            pltpu.VMEM((width, model), bf16),
            pltpu.VMEM((2, rows, half), f32),
            pltpu.VMEM((4, rows, half), bf16),
            pltpu.VMEM((2, rows, half), bf16),
        ),
        in_specs=[hbm] * 4,
        out_specs=(vmem,) * 5,
        scratch_shapes=[
            pltpu.VMEM((1, up_rows), f32),
            pltpu.VMEM(up_master.shape, f32),
            pltpu.VMEM(down_master.shape, f32),
            pltpu.VMEM((rows, model), bf16),
            pltpu.VMEM((down_rows, feats), bf16),
            pltpu.VMEM((starts, down_rows, feats), bf16),
            pltpu.VMEM((rows, 1), f32),
            pltpu.VMEM((rows, width), f32),
            pltpu.VMEM((rows, width), bf16),
            pltpu.VMEM((rows, half), f32),
            pltpu.VMEM((4, rows, half), bf16),
            pltpu.VMEM((2, rows, half), bf16),
            dma((3,)), dma((n_tp,)),
            dma((2, lines)), dma((lines, UP_CUTS)), dma((n_tp,)), dma((lines, 2)),
            dma((2, starts)), dma((8, starts, DOWN_CUTS)), dma((8,)),
            dma((2, starts)), dma((2, starts, DOWN_CUTS)), dma((starts, 2, DOWN_CUTS)),
            dma((4,)), dma((2,)), dma((7,)), dma((4,)),
        ],
        compiler_params=pltpu.CompilerParams(
            collective_id=0, has_side_effects=True, vmem_limit_bytes=VMEM_LIMIT * MIB
        ),
        cost_estimate=pl.CostEstimate(flops=flops, bytes_accessed=16 * MIB, transcendentals=0),
        name="layer",
    )(tokens, norm_gain[None, :], up_master, down_master)
    return pl.pallas_call(
        finish,
        out_shape=(
            jax.ShapeDtypeStruct((rows, feats), bf16),
            jax.ShapeDtypeStruct((depth, width), bf16),
            jax.ShapeDtypeStruct((width, model), bf16),
        ),
        in_specs=[vmem] * 5,
        out_specs=(hbm,) * 3,
        scratch_shapes=[pltpu.VMEM((rows, feats), bf16), dma((3,))],
        compiler_params=pltpu.CompilerParams(vmem_limit_bytes=8 * MIB),
        name="finish",
    )(*kept)


def solution(mesh):
    n, n_tp = mesh.shape["fs"], mesh.shape["tp"]
    return jax.shard_map(
        functools.partial(fused, n, n_tp),
        mesh=mesh,
        in_specs=(P("fs", "tp"), P("fs"), P("fs", "tp"), P("fs", "tp")),
        out_specs=(P("fs", "tp"), P(None, "tp"), P("tp", None)),
        check_vma=False,
    )
```

```python
import functools

import jax
import jax.numpy as jnp
from jax import lax
from jax.experimental import pallas as pl
from jax.experimental.pallas import tpu as pltpu
from jax.sharding import PartitionSpec as P

UP_CUTS = 2
DOWN_CUTS = 2
COLUMNS = 256
BOTH = 3
LANES = 128
VMEM_LIMIT = 46
MIB = 1024 * 1024


LINE, OVER, LAST, PASS, SHARE, TOKENS, SUM, SCALE, FINAL, TURN, CROSS = range(11)
END_OWN = (
    ((FINAL,), (PASS, 0, 0), (TOKENS,),),
    ((PASS, 0, 1),),
    ((LINE, 0, 0), (OVER, 0, 0),),
    ((LINE, 0, 1), (OVER, 0, 1),),
    ((LINE, 1, 0), (OVER, 1, 0), (LINE, 1, 1), (OVER, 1, 1), (TURN,),),
    ((LINE, 6, 1), (OVER, 6, 1), (PASS, 1, 0), (PASS, 1, 1),),
    ((LINE, 2, 0), (OVER, 2, 0), (LINE, 2, 1), (OVER, 2, 1), (LINE, 3, 0),
     (OVER, 3, 0), (LINE, 3, 1), (OVER, 3, 1), (CROSS, 0),),
    ((LINE, 4, 0), (OVER, 4, 0), (LINE, 4, 1), (OVER, 4, 1),),
    ((CROSS, 1), (LINE, 5, 0), (OVER, 5, 0), (LINE, 5, 1), (OVER, 5, 1),
     (LINE, 6, 0), (OVER, 6, 0),),
    ((LAST, 0, 0), (LAST, 1, 0),),
    ((LAST, 0, 1), (LAST, 1, 1),),
)
END_NEAR = (
    ((TOKENS,), (PASS, 0, 0),),
    ((PASS, 0, 1),),
    ((LINE, 0, 0), (OVER, 0, 0),),
    ((LINE, 0, 1), (OVER, 0, 1),),
    ((LINE, 1, 0), (OVER, 1, 0), (LINE, 1, 1), (OVER, 1, 1),),
    ((PASS, 1, 0), (PASS, 1, 1),),
    ((LINE, 2, 0), (OVER, 2, 0), (LINE, 2, 1), (OVER, 2, 1), (LINE, 3, 0),
     (OVER, 3, 0), (LINE, 3, 1), (OVER, 3, 1), (CROSS, 0),),
    ((LINE, 4, 0), (OVER, 4, 0), (LINE, 4, 1), (OVER, 4, 1),),
    ((CROSS, 1), (LINE, 5, 0), (OVER, 5, 0), (LINE, 5, 1), (OVER, 5, 1),
     (LINE, 6, 0), (OVER, 6, 0), (LINE, 6, 1), (OVER, 6, 1),),
    ((LAST, 0, 0), (LAST, 1, 0),),
    ((LAST, 0, 1), (LAST, 1, 1),),
)
END_FAR = (
    ((LINE, 0, 0), (OVER, 0, 0),),
    ((LINE, 0, 1), (OVER, 0, 1),),
    ((LINE, 1, 0), (OVER, 1, 0),),
    (),
    ((LINE, 1, 1), (OVER, 1, 1), (LINE, 2, 1), (OVER, 2, 1), (LINE, 2, 0),
     (OVER, 2, 0),),
    (),
    ((PASS, 0, 0), (PASS, 0, 1), (PASS, 1, 0), (PASS, 1, 1), (LINE, 3, 0),
     (OVER, 3, 0), (LINE, 3, 1), (OVER, 3, 1), (CROSS, 0),),
    ((LINE, 4, 0), (OVER, 4, 0), (LINE, 4, 1), (OVER, 4, 1),),
    ((CROSS, 1), (LINE, 5, 0), (OVER, 5, 0), (LINE, 5, 1), (OVER, 5, 1),
     (LINE, 6, 0), (OVER, 6, 0), (LINE, 6, 1), (OVER, 6, 1),),
    ((LAST, 0, 0), (LAST, 1, 0),),
    ((LAST, 0, 1), (LAST, 1, 1),),
)
IN_OWN = (
    ((FINAL,), (PASS, 0, 0), (PASS, 0, 1), (SHARE,), (LINE, 0, 0), (LINE, 0, 1),
     (OVER, 0, 0), (OVER, 0, 1), (LINE, 1, 0), (OVER, 1, 0), (LINE, 1, 1),
     (OVER, 1, 1), (TOKENS,), (SUM, 0), (PASS, 1, 0), (SUM, 1), (PASS, 1, 1),
     (SUM, 2), (LINE, 2, 0), (LINE, 2, 1), (OVER, 2, 0), (OVER, 2, 1),
     (LINE, 3, 0), (OVER, 3, 0), (LINE, 3, 1), (OVER, 3, 1), (LINE, 4, 0),
     (LINE, 4, 1), (LINE, 5, 0), (LINE, 5, 1), (LINE, 6, 0), (LINE, 6, 1),
     (SCALE,),),
    (),
    (),
    (),
    (),
    (),
    ((LAST, 0, 0), (LAST, 0, 1), (LAST, 1, 0), (LAST, 1, 1), (CROSS, 0),),
    ((OVER, 4, 0), (OVER, 4, 1), (TURN,),),
    ((CROSS, 1), (OVER, 5, 0), (OVER, 5, 1), (OVER, 6, 0), (OVER, 6, 1),),
    (),
    (),
)
IN_NEAR = (
    ((LINE, 0, 0), (LINE, 0, 1), (LINE, 2, 0), (LINE, 2, 1), (PASS, 0, 0),
     (PASS, 0, 1), (SHARE,), (OVER, 0, 0), (OVER, 0, 1), (LINE, 1, 0),
     (OVER, 1, 0), (LINE, 1, 1), (OVER, 1, 1), (TOKENS,), (SUM, 0), (PASS, 1, 0),
     (SUM, 1), (SUM, 2), (PASS, 1, 1), (OVER, 2, 0), (OVER, 2, 1), (LINE, 3, 0),
     (OVER, 3, 0), (LINE, 3, 1), (OVER, 3, 1), (LINE, 4, 0), (LINE, 4, 1),
     (LINE, 5, 0), (LINE, 5, 1), (LINE, 6, 0), (LINE, 6, 1), (SCALE,),),
    (),
    (),
    (),
    (),
    (),
    ((LAST, 0, 0), (LAST, 0, 1), (LAST, 1, 0), (LAST, 1, 1), (CROSS, 0),),
    ((OVER, 4, 0), (OVER, 4, 1),),
    ((CROSS, 1), (OVER, 5, 0), (OVER, 5, 1), (OVER, 6, 0), (OVER, 6, 1),),
    (),
    (),
)
IN_FAR = (
    ((PASS, 0, 0), (PASS, 0, 1), (PASS, 1, 0), (PASS, 1, 1), (SHARE,), (TOKENS,),
     (SUM, 0), (SUM, 1), (SUM, 2), (SCALE,), (LINE, 0, 0), (OVER, 0, 0),
     (LINE, 0, 1), (OVER, 0, 1),),
    ((LINE, 2, 0), (OVER, 2, 0),),
    ((LINE, 2, 1), (OVER, 2, 1),),
    ((LINE, 4, 0),),
    ((LINE, 4, 1), (LINE, 1, 0), (OVER, 1, 0), (LINE, 1, 1), (OVER, 1, 1),),
    ((LINE, 5, 0), (LINE, 5, 1),),
    ((LINE, 6, 0), (LINE, 6, 1), (LAST, 0, 0), (LAST, 0, 1), (LINE, 3, 0),
     (OVER, 3, 0), (LINE, 3, 1), (OVER, 3, 1), (CROSS, 0),),
    ((OVER, 4, 0), (OVER, 4, 1), (LAST, 1, 0), (LAST, 1, 1),),
    ((CROSS, 1), (OVER, 5, 0), (OVER, 5, 1), (OVER, 6, 0), (OVER, 6, 1),),
    (),
    (),
)


def kernel(
    n, n_tp,
    tokens_hbm, gain_hbm, upm_hbm, downm_hbm,
    up, down, own, take, crossed,
    gain_in, upm_in, downm_in, tok, shard, passing, scale, sums, hidden, kept, give, cross,
    tok_recv, gather_recv, up_send, upz_recv, upy_recv, both_recv,
    down_send, downz_recv, downy_recv, pass_send, pass_recv, last_recv,
    pair_recv, cross_recv, once_send, local_sem,
):
    f32, bf16 = jnp.float32, jnp.bfloat16
    f, t = lax.axis_index("fs"), lax.axis_index("tp")
    lines = n // 2
    z, y = f // 2, f % 2
    t1 = t + 1 - 2 * (t % 2)
    t2 = (t + 2) % 4
    t3 = (t1 + 2) % 4
    members = n // n_tp
    starts = members // 2
    owner = f // members
    above, below = (f + 2) % n, (f + n - 2) % n
    across = f + 1 - 2 * y
    has_above, has_below = z < lines - 1, z > 0
    upper, lower = t >= n_tp // 2, t < n_tp // 2
    at_end = jnp.logical_not(has_above & has_below)

    up_rows = upm_in.shape[0]
    down_rows = downm_in.shape[0]
    rows_all, feats = tokens_hbm.shape
    half = feats // 2
    width = up.shape[1]
    (up_over, down_over_send, last_over, gather_send, tok_send, pair_send, cross_send) = (
        once_send.at[i] for i in range(7)
    )
    dcut = down_rows // DOWN_CUTS
    first_cut = max(8, up_rows * BOTH // 128 * 8)
    ucuts = (first_cut, first_cut + (up_rows - first_cut) // 16 * 8, up_rows)

    def remote(src, dst, send, recv, **to):
        return pltpu.make_async_remote_copy(
            src_ref=src, dst_ref=dst, send_sem=send, recv_sem=recv,
            device_id=to, device_id_type=pl.DeviceIdType.MESH,
        )

    def down_block(source, column):
        rows = pl.ds(pl.multiple_of(source % members * down_rows, down_rows), down_rows)
        return down.at[rows, pl.ds(pl.multiple_of(column * feats, feats), feats)]

    loads = [
        pltpu.make_async_copy(upm_hbm, upm_in, local_sem.at[0]),
        pltpu.make_async_copy(gain_hbm, gain_in.at[0], local_sem.at[1]),
        pltpu.make_async_copy(downm_hbm, downm_in, local_sem.at[2]),
        pltpu.make_async_copy(
            tokens_hbm, tok.at[:, pl.ds(pl.multiple_of(t * feats, feats), feats)],
            local_sem.at[3],
        ),
    ]
    for load in loads:
        load.start()

    barrier = pltpu.get_barrier_semaphore()
    for other in (t1, t2, t3):
        pl.semaphore_signal(
            barrier, inc=1, device_id={"tp": other}, device_id_type=pl.DeviceIdType.MESH
        )
    pl.semaphore_signal(
        barrier, inc=1, device_id={"fs": across}, device_id_type=pl.DeviceIdType.MESH
    )

    @pl.when(has_above)
    def _():
        pl.semaphore_signal(
            barrier, inc=1, device_id={"fs": above}, device_id_type=pl.DeviceIdType.MESH
        )

    @pl.when(has_below)
    def _():
        pl.semaphore_signal(
            barrier, inc=1, device_id={"fs": below}, device_id_type=pl.DeviceIdType.MESH
        )

    loads[0].wait()
    loads[1].wait()
    gain = jnp.transpose(jnp.broadcast_to(gain_in[...], (LANES, up_rows)))
    for first in range(0, up.shape[1], LANES):
        up[pl.ds(pl.multiple_of(f * up_rows, up_rows), up_rows), pl.ds(first, LANES)] = (
            gain * upm_in[:, pl.ds(first, LANES)]
        ).astype(bf16)

    loads[2].wait()

    @pl.when(owner == t)
    def _():
        down_block(f, t)[...] = downm_in[...].astype(bf16)

    @pl.when(owner == t2)
    def _():
        passing[z % starts] = downm_in[...].astype(bf16)

    @pl.when((owner == t1) | (owner == t3))
    def _():
        shard[...] = downm_in[...].astype(bf16)

    pl.semaphore_wait(
        barrier, 4 + has_above.astype(jnp.int32) + has_below.astype(jnp.int32)
    )

    def up_piece(line, column, u):
        first, last = (ucuts[u], ucuts[u + 1]) if u >= 0 else (0, ucuts[0])
        row = (line * 2 + column) * up_rows + first
        return up.at[pl.ds(pl.multiple_of(row, 8), last - first), :]

    def both_copy(way, line, column, to):
        piece = up_piece(line, column, -1)
        return remote(
            piece, piece, up_over if way == 2 else up_send.at[way, line],
            both_recv.at[line, column], fs=to,
        )

    def spent(ref, send):
        remote(ref, ref, send, local_sem.at[0], fs=across).wait_send()

    def landed(ref, recv):
        remote(ref, ref, local_sem.at[0], recv, fs=across).wait_recv()

    def both_onward(line, column):
        @pl.when(has_above & (line <= z))
        def _():
            both_copy(0, line, column, above).start()

        @pl.when(has_below & (line >= z))
        def _():
            both_copy(1, line, column, below).start()

    def up_copy(way, line, u, to):
        piece = up_piece(line, y, u)
        if way == 2:
            return remote(piece, piece, up_over, upy_recv.at[line // starts], fs=to)
        return remote(piece, piece, up_send.at[way, line], upz_recv.at[line, u], fs=to)

    def up_onward(line, u):
        @pl.when(has_above & (line <= z))
        def _():
            up_copy(0, line, u, above).start()

        @pl.when(has_below & (line >= z))
        def _():
            up_copy(1, line, u, below).start()

        up_copy(2, line, u, across).start()

    both_copy(2, z, y, across).start()
    for u in range(UP_CUTS):
        up_onward(z, u)
    both_onward(z, y)

    def gather_copy(column, to):
        return remote(
            shard, down_block(f, column), gather_send, gather_recv.at[column], tp=to
        )

    order = ((t3, 0), (t2, 0), (t3, 1), (t2, 1), (t1, 0), (t1, 1), (t, 0), (t, 1))
    passed = (1, 3)
    finals = 7
    early = (0, 1, 2)

    passes_down = lower & has_below
    passes_up = upper & has_above

    def pass_copies(part, js, q, ways=(0, 1)):
        line = t2 * starts + js
        row = ((line * 2 + y) % members) * down_rows + q * dcut
        here = passing.at[js, pl.ds(q * dcut, dcut), pl.ds(part * half, half)]
        there = down.at[
            pl.ds(pl.multiple_of(row, dcut), dcut),
            pl.ds(pl.multiple_of(t * feats + part * half, half), half),
        ]

        def onward(to):
            remote(here, here, pass_send.at[0, js], pass_recv.at[part, js, q], fs=to).start()

        if 0 in ways:
            @pl.when(passes_down & (line >= z))
            def _():
                onward(below)

            @pl.when(passes_up & (line <= z))
            def _():
                onward(above)

        if 1 in ways:
            @pl.when((upper & (line <= z)) | (lower & (line >= z)))
            def _():
                remote(
                    here, there, pass_send.at[1, js], downz_recv.at[passed[part], js, q],
                    tp=t2,
                ).start()

    def pass_on(part, q):
        @pl.loop(0, starts)
        def _(js):
            line = t2 * starts + js

            @pl.when((upper & (line < z)) | (lower & (line > z)))
            def _():
                here = passing.at[js, pl.ds(q * dcut, dcut), pl.ds(part * half, half)]
                landed(here, pass_recv.at[part, js, q])
                pass_copies(part, js, q)

    def pass_start(way):
        @pl.when(owner == t2)
        def _():
            for part in range(2):
                for q in range(DOWN_CUTS):
                    pass_copies(part, z % starts, q, (way,))

    @pl.when((owner == t1) | (owner == t3))
    def _():
        gather_copy(t, owner).start()

    pass_start(1)
    loads[3].wait()

    def tok_copy(way, column, to):
        piece = tok.at[:, pl.ds(pl.multiple_of(column * feats, feats), feats)]
        return remote(piece, piece, tok_send, tok_recv.at[way], tp=to)

    tok_copy(1, t, t2).start()
    tok_copy(0, t, t1).start()

    sums[...] = jnp.zeros(sums.shape, f32)
    both_copy(2, z, 1 - y, across).wait_recv()
    both_onward(z, 1 - y)

    def both_relay(line, column):
        @pl.when((line >= 0) & (line < lines))
        def _():
            both_copy(0, line, column, above).wait_recv()
            both_onward(line, column)

    def down_piece(ci, js, side, q):
        column, part = order[ci]
        line = t * starts + js
        row = ((line * 2 + side) % members) * down_rows + q * dcut
        return down.at[
            pl.ds(pl.multiple_of(row, dcut), dcut),
            pl.ds(pl.multiple_of(column * feats + part * half, half), half),
        ]

    def down_copy(way, ci, js, q, to):
        piece = down_piece(ci, js, y, q)
        if way == 2:
            send = last_over if ci == finals else down_over_send
            return remote(piece, piece, send, downy_recv.at[ci], fs=to)
        return remote(piece, piece, down_send.at[way, js], downz_recv.at[ci, js, q], fs=to)

    def down_lines(ci, js, q):
        line = t * starts + js
        rising = has_above & (line <= z)
        falling = has_below & (line >= z)
        if ci in passed:
            rising = rising & upper
            falling = falling & lower
        else:
            rising = rising & (upper | (line < z))
            falling = falling & (lower | (line > z))

        @pl.when(rising)
        def _():
            down_copy(0, ci, js, q, above).start()

        @pl.when(falling)
        def _():
            down_copy(1, ci, js, q, below).start()

    def down_over(ci, js, q):
        if ci in early:
            @pl.when(t * starts + js != z)
            def _():
                down_copy(2, ci, js, q, across).start()
        else:
            down_copy(2, ci, js, q, across).start()

    def far_start():
        js = z % starts

        def send(make):
            @pl.when(lower & has_above)
            def _():
                make(0, above).start()

            @pl.when(upper & has_below)
            def _():
                make(1, below).start()

        @pl.when(owner == t)
        def _():
            for ci in (0, 2, 4, 5, 6):
                for q in range(DOWN_CUTS):
                    send(lambda way, to: down_copy(way, ci, js, q, to))
            for q in range(DOWN_CUTS):
                send(lambda way, to: last_copy(way, js, y, q, to))

    def last_copy(way, js, side, q, to):
        piece = down_piece(finals, js, side, q)
        return remote(
            piece, piece, down_send.at[way, js], last_recv.at[js, side, q], fs=to
        )

    def last_onward(js, side, q, sent=True):
        line = t * starts + js
        rising = has_above & (line <= z)
        falling = has_below & (line >= z)
        if sent:
            rising = rising & (upper | (line < z))
            falling = falling & (lower | (line > z))

        @pl.when(rising)
        def _():
            last_copy(0, js, side, q, above).start()

        @pl.when(falling)
        def _():
            last_copy(1, js, side, q, below).start()

    def relay(ci, q, ways=(0, 1)):
        @pl.loop(0, starts)
        def _(js):
            if 0 in ways or 2 in ways:
                if ci in passed and ci not in early:
                    down_copy(0, ci, js, q, above).wait_recv()
                else:
                    @pl.when(t * starts + js != z)
                    def _():
                        down_copy(0, ci, js, q, above).wait_recv()

            if 0 in ways:
                down_lines(ci, js, q)
            if 1 in ways:
                down_over(ci, js, q)

    def last_turn():
        @pl.when(owner == t)
        def _():
            js = z % starts
            landed(down.at[pl.ds(0, down_rows), pl.ds(0, half)], downy_recv.at[finals])
            for q in range(DOWN_CUTS):
                last_onward(js, 1 - y, q, False)
                last_onward(js, y, q)

    def last_relay(side, q):
        @pl.loop(0, starts)
        def _(js):
            @pl.when(t * starts + js != z)
            def _():
                last_copy(0, js, side, q, above).wait_recv()
                last_onward(js, side, q)

    def relayed(ci):
        landed(down.at[pl.ds(0, starts * down_rows), pl.ds(0, half)], downy_recv.at[ci])

    @pl.when(owner == t)
    def _():
        for ci in (4, 0):
            gather_copy(order[ci][0], t).wait_recv()

    @pl.when(at_end)
    def _():
        pass_start(0)
        far_start()

    step = min(rows_all, 128)
    low = (z < lines // 2).astype(jnp.int32)
    final = low * (n_tp - 1)

    inside = has_above & has_below
    near = (lower & (z < lines // 2)) | (upper & (z >= lines // 2))
    far = jnp.logical_not(near)

    def share():
        tok_copy(1, t2, t2).wait_recv()
        tok_copy(2, t2, t1).start()

    def scales():
        @pl.loop(0, rows_all // step)
        def _(i):
            rows = pl.ds(pl.multiple_of(i * step, step), step)
            values = tok[rows, :].astype(f32)
            mean_square = jnp.mean(values * values, axis=-1, keepdims=True)
            scale[rows, :] = lax.rsqrt(mean_square + 1e-06)

    def ordered(c):
        return low * c + (1 - low) * (n_tp - 1 - c)

    def reach(c):
        return ordered(c) * starts + starts - 1

    rest = up_rows - first_cut

    def arrived(c):
        landed(up.at[pl.ds(0, starts * rest), :], upy_recv.at[c])

    def before(c, columns):
        part = pl.ds(pl.multiple_of(c * feats, feats), feats)
        return jnp.dot(tok[:, part], up[part, columns], preferred_element_type=f32)

    def accumulate(c):
        arrived(c)

        @pl.loop(0, width // COLUMNS)
        def _(i):
            columns = pl.ds(pl.multiple_of(i * COLUMNS, COLUMNS), COLUMNS)
            sums[:, columns] += before(c, columns)

    def second():
        @pl.loop(0, n_tp)
        def _(c):
            @pl.when(reach(c) == lines - 2)
            def _():
                accumulate(c)

    @pl.loop(1, lines)
    def _(d):
        last = at_end & (d == lines - 1)

        def reached(c, step_c):
            @pl.loop(0, 2)
            def _(j):
                @pl.when(reach(c + j * step_c) <= lines - 3)
                def _():
                    accumulate(c + j * step_c)

        @pl.when(last)
        def _():
            tok_copy(0, t1, t1).wait_recv()
            reached(t, t1 - t)

        @pl.when(last & far)
        def _():
            share()
            tok_copy(2, t3, t1).wait_recv()
            reached(t2, t3 - t2)

        for u in range(UP_CUTS):
            @pl.when(z - d >= 0)
            def _():
                up_copy(0, z - d, u, above).wait_recv()
                up_onward(z - d, u)

            @pl.when(z + d < lines)
            def _():
                up_copy(1, z + d, u, below).wait_recv()
                up_onward(z + d, u)

            if u == 0:
                @pl.when(last & far)
                def _():
                    second()
                    scales()

                pl.when(last & near)(share)

        for column in (y, 1 - y):
            both_relay(z - d, column)
            both_relay(z + d, column)

        for k in range(len(early)):
            @pl.when((owner == t) & (d == k + 1))
            def _():
                for q in range(DOWN_CUTS):
                    if early[k] in passed:
                        down_copy(0, early[k], z % starts, q, above).wait_recv()
                    down_copy(2, early[k], z % starts, q, across).start()

    @pl.when(has_above & has_below)
    def _():
        pass_start(0)
        far_start()

    every = range(DOWN_CUTS)

    def final_over():
        for q in every:
            down_copy(2, finals, z % starts, q, across).start()

    def late_tokens():
        tok_copy(2, t3, t1).wait_recv()
        second()
        scales()

    def all_tokens():
        tok_copy(0, t1, t1).wait_recv()
        tok_copy(2, t3, t1).wait_recv()

    def product(ci):
        column, part = order[ci]
        first = pl.multiple_of(column * feats + part * half, half)
        return jnp.dot(hidden[...], down[:, pl.ds(first, half)], preferred_element_type=f32)

    def pair_copy(i):
        return remote(give.at[i], take.at[i], pair_send, pair_recv.at[i], tp=t1)

    def cross_copy(i):
        return remote(cross.at[i], crossed.at[i], cross_send, cross_recv.at[i], tp=t2)

    def cross_over(i):
        pair_copy(i).wait_recv()

        @pl.loop(0, rows_all // step)
        def _(j):
            rows = pl.ds(pl.multiple_of(j * step, step), step)
            cross[i, rows, :] = (kept[rows, :] + take[i, rows, :].astype(f32)).astype(bf16)

        cross_copy(i).start()

    def line_in(ci, q, end):
        relay(ci, q, (2,) if end else (0,))

    actions = {
        LINE: line_in,
        OVER: lambda ci, q, end: relay(ci, q, (1,)),
        LAST: lambda side, q, end: last_relay(y + side - 2 * y * side, q),
        PASS: lambda part, q, end: pass_on(part, q),
        SHARE: lambda end: share(),
        TOKENS: lambda end: late_tokens() if end else all_tokens(),
        SUM: lambda c, end: accumulate(ordered(c)),
        SCALE: lambda end: scales(),
        FINAL: lambda end: final_over(),
        TURN: lambda end: last_turn(),
        CROSS: lambda i, end: cross_over(i),
    }
    own_line = owner == t
    other_line = owner != t
    kinds = (
        (at_end & near & own_line, END_OWN), (at_end & near & other_line, END_NEAR),
        (at_end & far, END_FAR), (inside & near & own_line, IN_OWN),
        (inside & near & other_line, IN_NEAR), (inside & far, IN_FAR),
    )

    def slot(s):
        for kind, (condition, plan) in enumerate(kinds):
            def moves():
                for move, *args in plan[s]:
                    actions[move](*args, kind < 3)

            if plan[s]:
                pl.when(condition)(moves)

    slot(0)
    arrived(final)
    tiles = width // COLUMNS
    steps = 4
    for k in range(steps):
        @pl.loop(k * tiles // steps, (k + 1) * tiles // steps)
        def _(i):
            columns = pl.ds(pl.multiple_of(i * COLUMNS, COLUMNS), COLUMNS)
            value = jnp.maximum((sums[:, columns] + before(final, columns)) * scale[...], 0.0)
            hidden[:, columns] = (value * value).astype(bf16)

        slot(k + 1)

    def drain():
        @pl.loop(0, lines)
        def _(line):
            for way, onward in ((0, has_above & (line <= z)), (1, has_below & (line >= z))):
                @pl.when(onward)
                def _():
                    spent(up.at[pl.ds(0, up_rows + first_cut), :], up_send.at[way, line])

        spent(up.at[pl.ds(0, lines * rest + first_cut), :], up_over)

        @pl.loop(0, starts)
        def _(js):
            line = t2 * starts + js

            @pl.when((passes_down & (line >= z)) | (passes_up & (line <= z)))
            def _():
                spent(passing.at[js], pass_send.at[0, js])

            @pl.when((upper & (line <= z)) | (lower & (line >= z)))
            def _():
                spent(passing.at[js], pass_send.at[1, js])

        @pl.when((owner == t1) | (owner == t3))
        def _():
            spent(shard, gather_send)

        spent(tok.at[:, pl.ds(0, 3 * feats)], tok_send)

    def drain_down():
        @pl.loop(0, starts)
        def _(js):
            line = t * starts + js
            for way, onward, most in (
                (0, has_above & (line <= z), upper), (1, has_below & (line >= z), lower),
            ):
                for condition, pieces in ((most, 9), (jnp.logical_not(most), 7)):
                    @pl.when(onward & condition)
                    def _():
                        amount = pieces * down_rows // 8
                        spent(tok.at[pl.ds(0, amount), :], down_send.at[way, js])

        spent(down.at[pl.ds(0, starts * down_rows), pl.ds(0, 7 * half)], down_over_send)

        @pl.when(owner == t)
        def _():
            spent(down.at[pl.ds(0, down_rows), pl.ds(0, half)], last_over)

    relayed(0)
    give[0] = product(0).astype(bf16)
    pair_copy(0).start()
    slot(5)
    relayed(1)
    kept[...] = product(1)
    slot(6)
    relayed(2)
    give[1] = product(2).astype(bf16)
    pair_copy(1).start()
    slot(7)
    relayed(3)
    kept[...] = product(3)
    slot(8)
    relayed(4)
    give[2] = product(4).astype(bf16)
    pair_copy(2).start()
    slot(9)
    relayed(5)
    give[3] = product(5).astype(bf16)
    pair_copy(3).start()
    slot(10)
    drain()
    own[1] = product(7)
    if down_rows % LANES == 0:
        def partly(side):
            def term(js):
                part = pl.ds(
                    pl.multiple_of((2 * js + side) * down_rows, down_rows), down_rows
                )
                first = pl.multiple_of(t * feats, feats)
                return jnp.dot(
                    hidden[:, part], down[part, pl.ds(first, half)],
                    preferred_element_type=f32,
                )

            return sum((term(js) for js in range(1, starts)), term(0))

        own[0] = partly(y)
        relayed(6)
        own[0] += partly(1 - y)
    else:
        relayed(6)
        own[0] = product(6)
    for i in range(2):
        pair_copy(2 + i).wait_recv()
        cross_copy(i).wait_recv()

    drain_down()
    spent(give, pair_send)
    spent(cross, cross_send)


def finish(up, down, own, take, crossed, mixed_hbm, up_hbm, down_hbm, mixed, sems):
    copies = [
        pltpu.make_async_copy(up, up_hbm, sems.at[0]),
        pltpu.make_async_copy(down, down_hbm, sems.at[1]),
    ]
    for copy in copies:
        copy.start()
    rows_all, half = own.shape[1:]
    step = min(rows_all, 128)
    for i in range(2):
        @pl.loop(0, rows_all // step)
        def _(j):
            rows = pl.ds(pl.multiple_of(j * step, step), step)
            mixed[rows, pl.ds(i * half, half)] = (
                own[i, rows, :] + take[2 + i, rows, :].astype(jnp.float32)
                + crossed[i, rows, :].astype(jnp.float32)
            ).astype(mixed.dtype)

    copies.append(pltpu.make_async_copy(mixed, mixed_hbm, sems.at[2]))
    copies[2].start()
    for copy in copies:
        copy.wait()


def fused(n, n_tp, tokens, norm_gain, up_master, down_master):
    rows, feats = tokens.shape
    up_rows, width = up_master.shape
    down_rows = down_master.shape[0]
    depth = up_rows * n
    model = feats * n_tp
    half = feats // 2
    lines, starts = n // 2, n // n_tp // 2
    bf16, f32 = jnp.bfloat16, jnp.float32
    dma = pltpu.SemaphoreType.DMA
    vmem = pl.BlockSpec(memory_space=pltpu.VMEM)
    hbm = pl.BlockSpec(memory_space=pltpu.HBM)
    flops = 4 * rows * depth * width
    kept = pl.pallas_call(
        functools.partial(kernel, n, n_tp),
        out_shape=(
            pltpu.VMEM((depth, width), bf16),
            pltpu.VMEM((width, model), bf16),
            pltpu.VMEM((2, rows, half), f32),
            pltpu.VMEM((4, rows, half), bf16),
            pltpu.VMEM((2, rows, half), bf16),
        ),
        in_specs=[hbm] * 4,
        out_specs=(vmem,) * 5,
        scratch_shapes=[
            pltpu.VMEM((1, up_rows), f32),
            pltpu.VMEM(up_master.shape, f32),
            pltpu.VMEM(down_master.shape, f32),
            pltpu.VMEM((rows, model), bf16),
            pltpu.VMEM((down_rows, feats), bf16),
            pltpu.VMEM((starts, down_rows, feats), bf16),
            pltpu.VMEM((rows, 1), f32),
            pltpu.VMEM((rows, width), f32),
            pltpu.VMEM((rows, width), bf16),
            pltpu.VMEM((rows, half), f32),
            pltpu.VMEM((4, rows, half), bf16),
            pltpu.VMEM((2, rows, half), bf16),
            dma((3,)), dma((n_tp,)),
            dma((2, lines)), dma((lines, UP_CUTS)), dma((n_tp,)), dma((lines, 2)),
            dma((2, starts)), dma((8, starts, DOWN_CUTS)), dma((8,)),
            dma((2, starts)), dma((2, starts, DOWN_CUTS)), dma((starts, 2, DOWN_CUTS)),
            dma((4,)), dma((2,)), dma((7,)), dma((4,)),
        ],
        compiler_params=pltpu.CompilerParams(
            collective_id=0, has_side_effects=True, vmem_limit_bytes=VMEM_LIMIT * MIB
        ),
        cost_estimate=pl.CostEstimate(flops=flops, bytes_accessed=16 * MIB, transcendentals=0),
        name="layer",
    )(tokens, norm_gain, up_master, down_master)
    return pl.pallas_call(
        finish,
        out_shape=(
            jax.ShapeDtypeStruct((rows, feats), bf16),
            jax.ShapeDtypeStruct((depth, width), bf16),
            jax.ShapeDtypeStruct((width, model), bf16),
        ),
        in_specs=[vmem] * 5,
        out_specs=(hbm,) * 3,
        scratch_shapes=[pltpu.VMEM((rows, feats), bf16), dma((3,))],
        compiler_params=pltpu.CompilerParams(vmem_limit_bytes=8 * MIB),
        name="finish",
    )(*kept)


def solution(mesh):
    n, n_tp = mesh.shape["fs"], mesh.shape["tp"]
    return jax.shard_map(
        functools.partial(fused, n, n_tp),
        mesh=mesh,
        in_specs=(P("fs", "tp"), P("fs"), P("fs", "tp"), P("fs", "tp")),
        out_specs=(P("fs", "tp"), P(None, "tp"), P("tp", None)),
        check_vma=False,
    )
```

```python
import functools

import jax
import jax.numpy as jnp
from jax import lax
from jax.experimental import pallas as pl
from jax.experimental.pallas import tpu as pltpu
from jax.sharding import PartitionSpec as P

UP_CUTS = 2
DOWN_CUTS = 2
COLUMNS = 256
BOTH = 3
LANES = 128
VMEM_LIMIT = 46
MIB = 1024 * 1024


LINE, OVER, LAST, PASS, SHARE, TOKENS, SUM, SCALE, FINAL, TURN, CROSS = range(11)
END_OWN = (
    ((FINAL,), (PASS, 0, 0), (TOKENS,),),
    ((PASS, 0, 1),),
    ((LINE, 0, 0), (OVER, 0, 0),),
    ((LINE, 0, 1), (OVER, 0, 1),),
    ((LINE, 1, 0), (OVER, 1, 0), (LINE, 1, 1), (OVER, 1, 1), (TURN,),),
    ((LINE, 6, 1), (OVER, 6, 1), (PASS, 1, 1), (PASS, 1, 0), (LINE, 2, 0),),
    ((LINE, 2, 1), (OVER, 2, 1), (OVER, 2, 0), (LINE, 3, 0), (OVER, 3, 0),
     (LINE, 3, 1), (OVER, 3, 1), (CROSS, 0), (LINE, 4, 0), (OVER, 4, 0),),
    ((LINE, 4, 1), (OVER, 4, 1),),
    ((CROSS, 1), (LINE, 5, 0), (OVER, 5, 0), (LINE, 5, 1), (OVER, 5, 1),
     (LINE, 6, 0),),
    ((LAST, 0, 0), (LAST, 1, 0),),
    ((LAST, 0, 1), (LAST, 1, 1), (OVER, 6, 0),),
)
END_NEAR = (
    ((PASS, 0, 0), (TOKENS,),),
    ((PASS, 0, 1),),
    ((LINE, 0, 0), (OVER, 0, 0),),
    ((LINE, 0, 1), (OVER, 0, 1),),
    ((LINE, 1, 0), (OVER, 1, 0), (LINE, 1, 1), (OVER, 1, 1),),
    ((PASS, 1, 0), (PASS, 1, 1),),
    ((LINE, 2, 0), (OVER, 2, 0), (LINE, 2, 1), (OVER, 2, 1), (LINE, 3, 0),
     (OVER, 3, 0), (LINE, 3, 1), (OVER, 3, 1), (CROSS, 0),),
    ((LINE, 4, 0), (OVER, 4, 0), (LINE, 4, 1), (OVER, 4, 1),),
    ((CROSS, 1), (LINE, 5, 0), (OVER, 5, 0), (LINE, 5, 1), (OVER, 5, 1),
     (LINE, 6, 0), (OVER, 6, 0), (LINE, 6, 1), (OVER, 6, 1),),
    ((LAST, 0, 0), (LAST, 1, 0),),
    ((LAST, 0, 1), (LAST, 1, 1),),
)
END_FAR = (
    ((LINE, 0, 0), (OVER, 0, 0),),
    ((LINE, 0, 1), (OVER, 0, 1),),
    ((LINE, 1, 0), (OVER, 1, 0),),
    (),
    ((LINE, 1, 1), (OVER, 1, 1), (LINE, 2, 1), (OVER, 2, 1), (LINE, 2, 0),
     (OVER, 2, 0),),
    ((LINE, 4, 0),),
    ((PASS, 0, 0), (PASS, 0, 1), (PASS, 1, 0), (PASS, 1, 1), (CROSS, 0),
     (LINE, 3, 0), (OVER, 3, 0), (LINE, 3, 1), (OVER, 3, 1),),
    ((OVER, 4, 0), (LINE, 4, 1), (OVER, 4, 1),),
    ((CROSS, 1), (LINE, 5, 0), (OVER, 5, 0), (LINE, 5, 1), (OVER, 5, 1),
     (LINE, 6, 0), (OVER, 6, 0), (LINE, 6, 1), (OVER, 6, 1),),
    ((LAST, 0, 0), (LAST, 1, 0),),
    ((LAST, 0, 1), (LAST, 1, 1),),
)
IN_OWN = (
    ((PASS, 0, 0), (PASS, 0, 1), (SHARE,), (LINE, 0, 0), (LINE, 0, 1),
     (OVER, 0, 0), (OVER, 0, 1), (LINE, 1, 0), (OVER, 1, 0), (LINE, 1, 1),
     (OVER, 1, 1), (TOKENS,), (SUM, 0), (PASS, 1, 0), (SUM, 1), (PASS, 1, 1),
     (LINE, 2, 0), (LINE, 2, 1), (OVER, 2, 0), (LINE, 3, 0), (OVER, 3, 0),
     (OVER, 2, 1), (LINE, 3, 1), (SUM, 2), (OVER, 3, 1), (LINE, 4, 1),
     (LINE, 4, 0), (LINE, 5, 0), (LINE, 5, 1), (LINE, 6, 0), (LINE, 6, 1),
     (SCALE,),),
    ((FINAL,),),
    (),
    (),
    ((OVER, 4, 0), (OVER, 4, 1),),
    (),
    ((LAST, 0, 0), (LAST, 1, 0), (LAST, 1, 1), (CROSS, 0),),
    ((TURN,),),
    ((CROSS, 1), (OVER, 5, 0), (OVER, 5, 1), (LAST, 0, 1), (OVER, 6, 1),
     (OVER, 6, 0),),
    (),
    (),
)
IN_NEAR = (
    ((LINE, 0, 0), (LINE, 2, 0), (PASS, 0, 0), (LINE, 2, 1), (LINE, 0, 1),
     (PASS, 0, 1), (SHARE,), (OVER, 0, 0), (LINE, 1, 0), (OVER, 1, 0),
     (LINE, 1, 1), (OVER, 1, 1), (OVER, 0, 1), (TOKENS,), (SUM, 0), (SUM, 1),
     (PASS, 1, 1), (LINE, 3, 0), (OVER, 3, 0), (PASS, 1, 0), (LINE, 4, 0),
     (SUM, 2), (LINE, 3, 1), (OVER, 2, 0), (OVER, 2, 1), (OVER, 3, 1),
     (LINE, 4, 1), (LINE, 5, 0), (LINE, 5, 1), (LINE, 6, 0), (LINE, 6, 1),
     (SCALE,),),
    (),
    (),
    (),
    (),
    ((LAST, 0, 1),),
    ((LAST, 0, 0), (LAST, 1, 0), (LAST, 1, 1), (CROSS, 0),),
    (),
    ((OVER, 4, 0), (OVER, 4, 1), (CROSS, 1), (OVER, 5, 0), (OVER, 5, 1),
     (OVER, 6, 0), (OVER, 6, 1),),
    (),
    (),
)
IN_FAR = (
    ((PASS, 0, 1), (PASS, 1, 0), (PASS, 1, 1), (SHARE,), (TOKENS,), (SUM, 0),
     (SUM, 2), (SUM, 1), (SCALE,), (PASS, 0, 0), (LINE, 0, 0), (OVER, 0, 0),
     (LINE, 0, 1), (OVER, 0, 1),),
    ((LINE, 2, 0), (OVER, 2, 0),),
    ((LINE, 2, 1), (OVER, 2, 1),),
    ((LINE, 4, 0),),
    ((LINE, 1, 0), (LINE, 4, 1), (OVER, 1, 0), (LINE, 1, 1), (OVER, 1, 1),),
    ((LINE, 5, 0), (LINE, 5, 1), (OVER, 4, 0),),
    ((LINE, 6, 0), (LINE, 6, 1), (LAST, 0, 0), (LAST, 0, 1), (LINE, 3, 0),
     (OVER, 3, 0), (LINE, 3, 1), (OVER, 3, 1), (CROSS, 0),),
    ((OVER, 4, 1),),
    ((LAST, 1, 0), (CROSS, 1), (OVER, 5, 0), (OVER, 5, 1), (OVER, 6, 0),
     (OVER, 6, 1),),
    ((LAST, 1, 1),),
    (),
)


def kernel(
    n, n_tp,
    tokens_hbm, gain_hbm, upm_hbm, downm_hbm,
    up, down, own, take, crossed,
    gain_in, upm_in, downm_in, tok, shard, passing, scale, sums, hidden, kept, give, cross,
    tok_recv, gather_recv, up_send, upz_recv, upy_recv, both_recv,
    down_send, downz_recv, downy_recv, pass_send, pass_recv, last_recv,
    pair_recv, cross_recv, once_send, local_sem,
):
    f32, bf16 = jnp.float32, jnp.bfloat16
    f, t = lax.axis_index("fs"), lax.axis_index("tp")
    lines = n // 2
    z, y = f // 2, f % 2
    t1 = t + 1 - 2 * (t % 2)
    t2 = (t + 2) % 4
    t3 = (t1 + 2) % 4
    members = n // n_tp
    starts = members // 2
    owner = f // members
    above, below = (f + 2) % n, (f + n - 2) % n
    across = f + 1 - 2 * y
    has_above, has_below = z < lines - 1, z > 0
    upper, lower = t >= n_tp // 2, t < n_tp // 2
    at_end = jnp.logical_not(has_above & has_below)

    up_rows = upm_in.shape[0]
    down_rows = downm_in.shape[0]
    rows_all, feats = tokens_hbm.shape
    half = feats // 2
    width = up.shape[1]
    (up_over, down_over_send, last_over, gather_send, tok_send, pair_send, cross_send) = (
        once_send.at[i] for i in range(7)
    )
    dcut = down_rows // DOWN_CUTS
    first_cut = max(8, up_rows * BOTH // 128 * 8)
    ucuts = (first_cut, first_cut + (up_rows - first_cut) // 16 * 8, up_rows)

    def remote(src, dst, send, recv, **to):
        return pltpu.make_async_remote_copy(
            src_ref=src, dst_ref=dst, send_sem=send, recv_sem=recv,
            device_id=to, device_id_type=pl.DeviceIdType.MESH,
        )

    def down_block(source, column):
        rows = pl.ds(pl.multiple_of(source % members * down_rows, down_rows), down_rows)
        return down.at[rows, pl.ds(pl.multiple_of(column * feats, feats), feats)]

    loads = [
        pltpu.make_async_copy(upm_hbm, upm_in, local_sem.at[0]),
        pltpu.make_async_copy(gain_hbm, gain_in.at[0], local_sem.at[1]),
        pltpu.make_async_copy(downm_hbm, downm_in, local_sem.at[2]),
        pltpu.make_async_copy(
            tokens_hbm, tok.at[:, pl.ds(pl.multiple_of(t * feats, feats), feats)],
            local_sem.at[3],
        ),
    ]
    for load in loads:
        load.start()

    barrier = pltpu.get_barrier_semaphore()
    for other in (t1, t2, t3):
        pl.semaphore_signal(
            barrier, inc=1, device_id={"tp": other}, device_id_type=pl.DeviceIdType.MESH
        )
    pl.semaphore_signal(
        barrier, inc=1, device_id={"fs": across}, device_id_type=pl.DeviceIdType.MESH
    )

    @pl.when(has_above)
    def _():
        pl.semaphore_signal(
            barrier, inc=1, device_id={"fs": above}, device_id_type=pl.DeviceIdType.MESH
        )

    @pl.when(has_below)
    def _():
        pl.semaphore_signal(
            barrier, inc=1, device_id={"fs": below}, device_id_type=pl.DeviceIdType.MESH
        )

    loads[0].wait()
    loads[1].wait()
    gain = jnp.transpose(jnp.broadcast_to(gain_in[...], (LANES, up_rows)))
    for first in range(0, up.shape[1], LANES):
        up[pl.ds(pl.multiple_of(f * up_rows, up_rows), up_rows), pl.ds(first, LANES)] = (
            gain * upm_in[:, pl.ds(first, LANES)]
        ).astype(bf16)

    loads[2].wait()

    @pl.when(owner == t)
    def _():
        down_block(f, t)[...] = downm_in[...].astype(bf16)

    @pl.when(owner == t2)
    def _():
        passing[z % starts] = downm_in[...].astype(bf16)

    @pl.when((owner == t1) | (owner == t3))
    def _():
        shard[...] = downm_in[...].astype(bf16)

    pl.semaphore_wait(
        barrier, 4 + has_above.astype(jnp.int32) + has_below.astype(jnp.int32)
    )

    def up_piece(line, column, u):
        first, last = (ucuts[u], ucuts[u + 1]) if u >= 0 else (0, ucuts[0])
        row = (line * 2 + column) * up_rows + first
        return up.at[pl.ds(pl.multiple_of(row, 8), last - first), :]

    def both_copy(way, line, column, to):
        piece = up_piece(line, column, -1)
        return remote(
            piece, piece, up_over if way == 2 else up_send.at[way, line],
            both_recv.at[line, column], fs=to,
        )

    def spent(ref, send):
        remote(ref, ref, send, local_sem.at[0], fs=across).wait_send()

    def landed(ref, recv):
        remote(ref, ref, local_sem.at[0], recv, fs=across).wait_recv()

    def both_onward(line, column):
        @pl.when(has_above & (line <= z))
        def _():
            both_copy(0, line, column, above).start()

        @pl.when(has_below & (line >= z))
        def _():
            both_copy(1, line, column, below).start()

    def up_copy(way, line, u, to):
        piece = up_piece(line, y, u)
        if way == 2:
            return remote(piece, piece, up_over, upy_recv.at[line // starts], fs=to)
        return remote(piece, piece, up_send.at[way, line], upz_recv.at[line, u], fs=to)

    def up_onward(line, u):
        @pl.when(has_above & (line <= z))
        def _():
            up_copy(0, line, u, above).start()

        @pl.when(has_below & (line >= z))
        def _():
            up_copy(1, line, u, below).start()

        up_copy(2, line, u, across).start()

    both_copy(2, z, y, across).start()
    for u in range(UP_CUTS):
        up_onward(z, u)
    both_onward(z, y)

    def gather_copy(column, to):
        return remote(
            shard, down_block(f, column), gather_send, gather_recv.at[column], tp=to
        )

    order = ((t3, 0), (t2, 0), (t3, 1), (t2, 1), (t1, 0), (t1, 1), (t, 0), (t, 1))
    passed = (1, 3)
    finals = 7
    early = (0, 1, 2)

    passes_down = lower & has_below
    passes_up = upper & has_above

    def pass_copies(part, js, q, ways=(0, 1)):
        line = t2 * starts + js
        row = ((line * 2 + y) % members) * down_rows + q * dcut
        here = passing.at[js, pl.ds(q * dcut, dcut), pl.ds(part * half, half)]
        there = down.at[
            pl.ds(pl.multiple_of(row, dcut), dcut),
            pl.ds(pl.multiple_of(t * feats + part * half, half), half),
        ]

        def onward(to):
            remote(here, here, pass_send.at[0, js], pass_recv.at[part, js, q], fs=to).start()

        if 0 in ways:
            @pl.when(passes_down & (line >= z))
            def _():
                onward(below)

            @pl.when(passes_up & (line <= z))
            def _():
                onward(above)

        if 1 in ways:
            @pl.when((upper & (line <= z)) | (lower & (line >= z)))
            def _():
                remote(
                    here, there, pass_send.at[1, js], downz_recv.at[passed[part], js, q],
                    tp=t2,
                ).start()

    def pass_on(part, q):
        @pl.loop(0, starts)
        def _(js):
            line = t2 * starts + js

            @pl.when((upper & (line < z)) | (lower & (line > z)))
            def _():
                here = passing.at[js, pl.ds(q * dcut, dcut), pl.ds(part * half, half)]
                landed(here, pass_recv.at[part, js, q])
                pass_copies(part, js, q)

    def pass_start(way):
        @pl.when(owner == t2)
        def _():
            for part in range(2):
                for q in range(DOWN_CUTS):
                    pass_copies(part, z % starts, q, (way,))

    @pl.when((owner == t1) | (owner == t3))
    def _():
        gather_copy(t, owner).start()

    pass_start(1)
    loads[3].wait()

    def tok_copy(way, column, to):
        piece = tok.at[:, pl.ds(pl.multiple_of(column * feats, feats), feats)]
        return remote(piece, piece, tok_send, tok_recv.at[way], tp=to)

    tok_copy(1, t, t2).start()
    tok_copy(0, t, t1).start()

    sums[...] = jnp.zeros(sums.shape, f32)
    both_copy(2, z, 1 - y, across).wait_recv()
    both_onward(z, 1 - y)

    def both_relay(line, column):
        @pl.when((line >= 0) & (line < lines))
        def _():
            both_copy(0, line, column, above).wait_recv()
            both_onward(line, column)

    def down_piece(ci, js, side, q):
        column, part = order[ci]
        line = t * starts + js
        row = ((line * 2 + side) % members) * down_rows + q * dcut
        return down.at[
            pl.ds(pl.multiple_of(row, dcut), dcut),
            pl.ds(pl.multiple_of(column * feats + part * half, half), half),
        ]

    def down_copy(way, ci, js, q, to):
        piece = down_piece(ci, js, y, q)
        if way == 2:
            send = last_over if ci == finals else down_over_send
            return remote(piece, piece, send, downy_recv.at[ci], fs=to)
        return remote(piece, piece, down_send.at[way, js], downz_recv.at[ci, js, q], fs=to)

    def down_lines(ci, js, q):
        line = t * starts + js
        rising = has_above & (line <= z)
        falling = has_below & (line >= z)
        if ci in passed:
            rising = rising & upper
            falling = falling & lower
        else:
            rising = rising & (upper | (line < z))
            falling = falling & (lower | (line > z))

        @pl.when(rising)
        def _():
            down_copy(0, ci, js, q, above).start()

        @pl.when(falling)
        def _():
            down_copy(1, ci, js, q, below).start()

    def down_over(ci, js, q):
        if ci in early:
            @pl.when(t * starts + js != z)
            def _():
                down_copy(2, ci, js, q, across).start()
        else:
            down_copy(2, ci, js, q, across).start()

    def far_start():
        js = z % starts

        def send(make):
            @pl.when(lower & has_above)
            def _():
                make(0, above).start()

            @pl.when(upper & has_below)
            def _():
                make(1, below).start()

        @pl.when(owner == t)
        def _():
            for ci in (0, 2, 4, 5, 6):
                for q in range(DOWN_CUTS):
                    send(lambda way, to: down_copy(way, ci, js, q, to))
            for q in range(DOWN_CUTS):
                send(lambda way, to: last_copy(way, js, y, q, to))

    def last_copy(way, js, side, q, to):
        piece = down_piece(finals, js, side, q)
        return remote(
            piece, piece, down_send.at[way, js], last_recv.at[js, side, q], fs=to
        )

    def last_onward(js, side, q, sent=True):
        line = t * starts + js
        rising = has_above & (line <= z)
        falling = has_below & (line >= z)
        if sent:
            rising = rising & (upper | (line < z))
            falling = falling & (lower | (line > z))

        @pl.when(rising)
        def _():
            last_copy(0, js, side, q, above).start()

        @pl.when(falling)
        def _():
            last_copy(1, js, side, q, below).start()

    def relay(ci, q, ways=(0, 1)):
        @pl.loop(0, starts)
        def _(js):
            if 0 in ways or 2 in ways:
                if ci in passed and ci not in early:
                    down_copy(0, ci, js, q, above).wait_recv()
                else:
                    @pl.when(t * starts + js != z)
                    def _():
                        down_copy(0, ci, js, q, above).wait_recv()

            if 0 in ways:
                down_lines(ci, js, q)
            if 1 in ways:
                down_over(ci, js, q)

    def last_turn():
        @pl.when(owner == t)
        def _():
            js = z % starts
            landed(down.at[pl.ds(0, down_rows), pl.ds(0, half)], downy_recv.at[finals])
            for q in range(DOWN_CUTS):
                last_onward(js, 1 - y, q, False)
                last_onward(js, y, q)

    def last_relay(side, q):
        @pl.loop(0, starts)
        def _(js):
            @pl.when(t * starts + js != z)
            def _():
                last_copy(0, js, side, q, above).wait_recv()
                last_onward(js, side, q)

    def relayed(ci):
        landed(down.at[pl.ds(0, starts * down_rows), pl.ds(0, half)], downy_recv.at[ci])

    @pl.when(owner == t)
    def _():
        for ci in (4, 0):
            gather_copy(order[ci][0], t).wait_recv()

    @pl.when(at_end)
    def _():
        pass_start(0)
        far_start()

    step = min(rows_all, 128)
    low = (z < lines // 2).astype(jnp.int32)
    final = low * (n_tp - 1)

    inside = has_above & has_below
    near = (lower & (z < lines // 2)) | (upper & (z >= lines // 2))
    far = jnp.logical_not(near)

    def share():
        tok_copy(1, t2, t2).wait_recv()
        tok_copy(2, t2, t1).start()

    def scales():
        @pl.loop(0, rows_all // step)
        def _(i):
            rows = pl.ds(pl.multiple_of(i * step, step), step)
            values = tok[rows, :].astype(f32)
            mean_square = jnp.mean(values * values, axis=-1, keepdims=True)
            scale[rows, :] = lax.rsqrt(mean_square + 1e-06)

    def ordered(c):
        return low * c + (1 - low) * (n_tp - 1 - c)

    def reach(c):
        return ordered(c) * starts + starts - 1

    rest = up_rows - first_cut

    def arrived(c):
        landed(up.at[pl.ds(0, starts * rest), :], upy_recv.at[c])

    def before(c, columns):
        part = pl.ds(pl.multiple_of(c * feats, feats), feats)
        return jnp.dot(tok[:, part], up[part, columns], preferred_element_type=f32)

    def accumulate(c):
        arrived(c)

        @pl.loop(0, width // COLUMNS)
        def _(i):
            columns = pl.ds(pl.multiple_of(i * COLUMNS, COLUMNS), COLUMNS)
            sums[:, columns] += before(c, columns)

    def second():
        @pl.loop(0, n_tp)
        def _(c):
            @pl.when(reach(c) == lines - 2)
            def _():
                accumulate(c)

    @pl.loop(1, lines)
    def _(d):
        last = at_end & (d == lines - 1)

        def reached(c, step_c):
            @pl.loop(0, 2)
            def _(j):
                @pl.when(reach(c + j * step_c) <= lines - 3)
                def _():
                    accumulate(c + j * step_c)

        @pl.when(last)
        def _():
            tok_copy(0, t1, t1).wait_recv()
            reached(t, t1 - t)

        @pl.when(last & far)
        def _():
            share()
            tok_copy(2, t3, t1).wait_recv()
            reached(t2, t3 - t2)

        for u in range(UP_CUTS):
            @pl.when(z - d >= 0)
            def _():
                up_copy(0, z - d, u, above).wait_recv()
                up_onward(z - d, u)

            @pl.when(z + d < lines)
            def _():
                up_copy(1, z + d, u, below).wait_recv()
                up_onward(z + d, u)

            if u == 0:
                @pl.when(last & far)
                def _():
                    second()
                    scales()

                pl.when(last & near)(share)

        for column in (y, 1 - y):
            both_relay(z - d, column)
            both_relay(z + d, column)

        for k in range(len(early)):
            @pl.when((owner == t) & (d == k + 1))
            def _():
                for q in range(DOWN_CUTS):
                    if early[k] in passed:
                        down_copy(0, early[k], z % starts, q, above).wait_recv()
                    down_copy(2, early[k], z % starts, q, across).start()

    @pl.when(has_above & has_below)
    def _():
        pass_start(0)
        far_start()

    every = range(DOWN_CUTS)

    def final_over():
        for q in every:
            down_copy(2, finals, z % starts, q, across).start()

    def late_tokens():
        tok_copy(2, t3, t1).wait_recv()
        second()
        scales()

    def all_tokens():
        tok_copy(0, t1, t1).wait_recv()
        tok_copy(2, t3, t1).wait_recv()

    def product(ci):
        column, part = order[ci]
        first = pl.multiple_of(column * feats + part * half, half)
        return jnp.dot(hidden[...], down[:, pl.ds(first, half)], preferred_element_type=f32)

    def pair_copy(i):
        return remote(give.at[i], take.at[i], pair_send, pair_recv.at[i], tp=t1)

    def cross_copy(i):
        return remote(cross.at[i], crossed.at[i], cross_send, cross_recv.at[i], tp=t2)

    def cross_over(i):
        pair_copy(i).wait_recv()

        @pl.loop(0, rows_all // step)
        def _(j):
            rows = pl.ds(pl.multiple_of(j * step, step), step)
            cross[i, rows, :] = (kept[rows, :] + take[i, rows, :].astype(f32)).astype(bf16)

        cross_copy(i).start()

    def line_in(ci, q, end):
        relay(ci, q, (2,) if end else (0,))

    actions = {
        LINE: line_in,
        OVER: lambda ci, q, end: relay(ci, q, (1,)),
        LAST: lambda side, q, end: last_relay(y + side - 2 * y * side, q),
        PASS: lambda part, q, end: pass_on(part, q),
        SHARE: lambda end: share(),
        TOKENS: lambda end: late_tokens() if end else all_tokens(),
        SUM: lambda c, end: accumulate(ordered(c)),
        SCALE: lambda end: scales(),
        FINAL: lambda end: final_over(),
        TURN: lambda end: last_turn(),
        CROSS: lambda i, end: cross_over(i),
    }
    own_line = owner == t
    other_line = owner != t
    kinds = (
        (at_end & near & own_line, END_OWN), (at_end & near & other_line, END_NEAR),
        (at_end & far, END_FAR), (inside & near & own_line, IN_OWN),
        (inside & near & other_line, IN_NEAR), (inside & far, IN_FAR),
    )

    def slot(s):
        for kind, (condition, plan) in enumerate(kinds):
            def moves():
                for move, *args in plan[s]:
                    actions[move](*args, kind < 3)

            if plan[s]:
                pl.when(condition)(moves)

    slot(0)
    arrived(final)
    tiles = width // COLUMNS
    steps = 4
    for k in range(steps):
        @pl.loop(k * tiles // steps, (k + 1) * tiles // steps)
        def _(i):
            columns = pl.ds(pl.multiple_of(i * COLUMNS, COLUMNS), COLUMNS)
            value = jnp.maximum((sums[:, columns] + before(final, columns)) * scale[...], 0.0)
            hidden[:, columns] = (value * value).astype(bf16)

        slot(k + 1)

    def drain():
        @pl.loop(0, lines)
        def _(line):
            for way, onward in ((0, has_above & (line <= z)), (1, has_below & (line >= z))):
                @pl.when(onward)
                def _():
                    spent(up.at[pl.ds(0, up_rows + first_cut), :], up_send.at[way, line])

        spent(up.at[pl.ds(0, lines * rest + first_cut), :], up_over)

        @pl.loop(0, starts)
        def _(js):
            line = t2 * starts + js

            @pl.when((passes_down & (line >= z)) | (passes_up & (line <= z)))
            def _():
                spent(passing.at[js], pass_send.at[0, js])

            @pl.when((upper & (line <= z)) | (lower & (line >= z)))
            def _():
                spent(passing.at[js], pass_send.at[1, js])

        @pl.when((owner == t1) | (owner == t3))
        def _():
            spent(shard, gather_send)

        spent(tok.at[:, pl.ds(0, 3 * feats)], tok_send)

    def drain_down():
        @pl.loop(0, starts)
        def _(js):
            line = t * starts + js
            for way, onward, most in (
                (0, has_above & (line <= z), upper), (1, has_below & (line >= z), lower),
            ):
                for condition, pieces in ((most, 9), (jnp.logical_not(most), 7)):
                    @pl.when(onward & condition)
                    def _():
                        amount = pieces * down_rows // 8
                        spent(tok.at[pl.ds(0, amount), :], down_send.at[way, js])

        spent(down.at[pl.ds(0, starts * down_rows), pl.ds(0, 7 * half)], down_over_send)

        @pl.when(owner == t)
        def _():
            spent(down.at[pl.ds(0, down_rows), pl.ds(0, half)], last_over)

    relayed(0)
    give[0] = product(0).astype(bf16)
    pair_copy(0).start()
    slot(5)
    relayed(1)
    kept[...] = product(1)
    slot(6)
    relayed(2)
    give[1] = product(2).astype(bf16)
    pair_copy(1).start()
    slot(7)
    relayed(3)
    kept[...] = product(3)
    slot(8)
    relayed(4)
    give[2] = product(4).astype(bf16)
    pair_copy(2).start()
    slot(9)
    relayed(5)
    give[3] = product(5).astype(bf16)
    pair_copy(3).start()
    slot(10)
    drain()
    own[1] = product(7)
    if down_rows % LANES == 0:
        def partly(side):
            def term(js):
                part = pl.ds(
                    pl.multiple_of((2 * js + side) * down_rows, down_rows), down_rows
                )
                first = pl.multiple_of(t * feats, feats)
                return jnp.dot(
                    hidden[:, part], down[part, pl.ds(first, half)],
                    preferred_element_type=f32,
                )

            return sum((term(js) for js in range(1, starts)), term(0))

        own[0] = partly(y)
        relayed(6)
        own[0] += partly(1 - y)
    else:
        relayed(6)
        own[0] = product(6)
    for i in range(2):
        pair_copy(2 + i).wait_recv()
        cross_copy(i).wait_recv()

    drain_down()
    spent(give, pair_send)
    spent(cross, cross_send)


def finish(up, down, own, take, crossed, mixed_hbm, up_hbm, down_hbm, mixed, sems):
    copies = [
        pltpu.make_async_copy(up, up_hbm, sems.at[0]),
        pltpu.make_async_copy(down, down_hbm, sems.at[1]),
    ]
    for copy in copies:
        copy.start()
    rows_all, half = own.shape[1:]
    step = min(rows_all, 128)
    for i in range(2):
        @pl.loop(0, rows_all // step)
        def _(j):
            rows = pl.ds(pl.multiple_of(j * step, step), step)
            mixed[rows, pl.ds(i * half, half)] = (
                own[i, rows, :] + take[2 + i, rows, :].astype(jnp.float32)
                + crossed[i, rows, :].astype(jnp.float32)
            ).astype(mixed.dtype)

    copies.append(pltpu.make_async_copy(mixed, mixed_hbm, sems.at[2]))
    copies[2].start()
    for copy in copies:
        copy.wait()


def fused(n, n_tp, tokens, norm_gain, up_master, down_master):
    rows, feats = tokens.shape
    up_rows, width = up_master.shape
    down_rows = down_master.shape[0]
    depth = up_rows * n
    model = feats * n_tp
    half = feats // 2
    lines, starts = n // 2, n // n_tp // 2
    bf16, f32 = jnp.bfloat16, jnp.float32
    dma = pltpu.SemaphoreType.DMA
    vmem = pl.BlockSpec(memory_space=pltpu.VMEM)
    hbm = pl.BlockSpec(memory_space=pltpu.HBM)
    flops = 4 * rows * depth * width
    kept = pl.pallas_call(
        functools.partial(kernel, n, n_tp),
        out_shape=(
            pltpu.VMEM((depth, width), bf16),
            pltpu.VMEM((width, model), bf16),
            pltpu.VMEM((2, rows, half), f32),
            pltpu.VMEM((4, rows, half), bf16),
            pltpu.VMEM((2, rows, half), bf16),
        ),
        in_specs=[hbm] * 4,
        out_specs=(vmem,) * 5,
        scratch_shapes=[
            pltpu.VMEM((1, up_rows), f32),
            pltpu.VMEM(up_master.shape, f32),
            pltpu.VMEM(down_master.shape, f32),
            pltpu.VMEM((rows, model), bf16),
            pltpu.VMEM((down_rows, feats), bf16),
            pltpu.VMEM((starts, down_rows, feats), bf16),
            pltpu.VMEM((rows, 1), f32),
            pltpu.VMEM((rows, width), f32),
            pltpu.VMEM((rows, width), bf16),
            pltpu.VMEM((rows, half), f32),
            pltpu.VMEM((4, rows, half), bf16),
            pltpu.VMEM((2, rows, half), bf16),
            dma((3,)), dma((n_tp,)),
            dma((2, lines)), dma((lines, UP_CUTS)), dma((n_tp,)), dma((lines, 2)),
            dma((2, starts)), dma((8, starts, DOWN_CUTS)), dma((8,)),
            dma((2, starts)), dma((2, starts, DOWN_CUTS)), dma((starts, 2, DOWN_CUTS)),
            dma((4,)), dma((2,)), dma((7,)), dma((4,)),
        ],
        compiler_params=pltpu.CompilerParams(
            collective_id=0, has_side_effects=True, vmem_limit_bytes=VMEM_LIMIT * MIB
        ),
        cost_estimate=pl.CostEstimate(flops=flops, bytes_accessed=16 * MIB, transcendentals=0),
        name="layer",
    )(tokens, norm_gain, up_master, down_master)
    return pl.pallas_call(
        finish,
        out_shape=(
            jax.ShapeDtypeStruct((rows, feats), bf16),
            jax.ShapeDtypeStruct((depth, width), bf16),
            jax.ShapeDtypeStruct((width, model), bf16),
        ),
        in_specs=[vmem] * 5,
        out_specs=(hbm,) * 3,
        scratch_shapes=[pltpu.VMEM((rows, feats), bf16), dma((3,))],
        compiler_params=pltpu.CompilerParams(vmem_limit_bytes=8 * MIB),
        name="finish",
    )(*kept)


def solution(mesh):
    n, n_tp = mesh.shape["fs"], mesh.shape["tp"]
    return jax.shard_map(
        functools.partial(fused, n, n_tp),
        mesh=mesh,
        in_specs=(P("fs", "tp"), P("fs"), P("fs", "tp"), P("fs", "tp")),
        out_specs=(P("fs", "tp"), P(None, "tp"), P("tp", None)),
        check_vma=False,
    )
```

```python
import functools

import jax
import jax.numpy as jnp
from jax import lax
from jax.experimental import pallas as pl
from jax.experimental.pallas import tpu as pltpu
from jax.sharding import PartitionSpec as P

UP_CUTS = 2
DOWN_CUTS = 2
COLUMNS = 256
BOTH = 3
LANES = 128
VMEM_LIMIT = 46
MIB = 1024 * 1024


LINE, OVER, LAST, PASS, SHARE, TOKENS, SUM, SCALE, FINAL, TURN, CROSS = range(11)
END_OWN = (
    ((FINAL,), (PASS, 0, 0), (TOKENS,),),
    ((PASS, 0, 1),),
    ((LINE, 0, 0), (OVER, 0, 0),),
    ((LINE, 0, 1), (OVER, 0, 1),),
    ((LINE, 1, 0), (OVER, 1, 0), (LINE, 1, 1), (OVER, 1, 1), (TURN,),),
    ((LINE, 6, 1), (OVER, 6, 1), (PASS, 1, 1), (PASS, 1, 0), (LINE, 2, 0),),
    ((LINE, 2, 1), (OVER, 2, 1), (OVER, 2, 0), (LINE, 3, 0), (OVER, 3, 0),
     (LINE, 3, 1), (OVER, 3, 1), (CROSS, 0), (LINE, 4, 0), (OVER, 4, 0),),
    ((LINE, 4, 1), (OVER, 4, 1),),
    ((CROSS, 1), (LINE, 5, 0), (OVER, 5, 0), (LINE, 5, 1), (OVER, 5, 1),
     (LINE, 6, 0),),
    ((LAST, 0, 0), (LAST, 1, 0),),
    ((LAST, 0, 1), (LAST, 1, 1), (OVER, 6, 0),),
)
END_NEAR = (
    ((PASS, 0, 0), (TOKENS,),),
    ((PASS, 0, 1),),
    ((LINE, 0, 0), (OVER, 0, 0),),
    ((LINE, 0, 1), (OVER, 0, 1),),
    ((LINE, 1, 0), (OVER, 1, 0), (LINE, 1, 1), (OVER, 1, 1),),
    ((PASS, 1, 0), (PASS, 1, 1),),
    ((LINE, 2, 0), (OVER, 2, 0), (LINE, 2, 1), (OVER, 2, 1), (LINE, 3, 0),
     (OVER, 3, 0), (LINE, 3, 1), (OVER, 3, 1), (CROSS, 0),),
    ((LINE, 4, 0), (OVER, 4, 0), (LINE, 4, 1), (OVER, 4, 1),),
    ((CROSS, 1), (LINE, 5, 0), (OVER, 5, 0), (LINE, 5, 1), (OVER, 5, 1),
     (LINE, 6, 0), (OVER, 6, 0), (LINE, 6, 1), (OVER, 6, 1),),
    ((LAST, 0, 0), (LAST, 1, 0),),
    ((LAST, 0, 1), (LAST, 1, 1),),
)
END_FAR = (
    ((LINE, 0, 0), (OVER, 0, 0),),
    ((LINE, 0, 1), (OVER, 0, 1),),
    ((LINE, 1, 0), (OVER, 1, 0),),
    (),
    ((LINE, 1, 1), (OVER, 1, 1), (LINE, 2, 1), (OVER, 2, 1), (LINE, 2, 0),
     (OVER, 2, 0),),
    ((LINE, 4, 0),),
    ((PASS, 0, 0), (PASS, 0, 1), (PASS, 1, 0), (PASS, 1, 1), (CROSS, 0),
     (LINE, 3, 0), (OVER, 3, 0), (LINE, 3, 1), (OVER, 3, 1),),
    ((OVER, 4, 0), (LINE, 4, 1), (OVER, 4, 1),),
    ((CROSS, 1), (LINE, 5, 0), (OVER, 5, 0), (LINE, 5, 1), (OVER, 5, 1),
     (LINE, 6, 0), (OVER, 6, 0), (LINE, 6, 1), (OVER, 6, 1),),
    ((LAST, 0, 0), (LAST, 1, 0),),
    ((LAST, 0, 1), (LAST, 1, 1),),
)
IN_OWN = (
    ((PASS, 0, 0), (PASS, 0, 1), (SHARE,), (LINE, 0, 0), (LINE, 0, 1),
     (OVER, 0, 0), (OVER, 0, 1), (LINE, 1, 0), (OVER, 1, 0), (LINE, 1, 1),
     (OVER, 1, 1), (TOKENS,), (SUM, 0), (PASS, 1, 0), (SUM, 1), (PASS, 1, 1),
     (LINE, 2, 0), (LINE, 2, 1), (OVER, 2, 0), (LINE, 3, 0), (OVER, 3, 0),
     (OVER, 2, 1), (LINE, 3, 1), (SUM, 2), (OVER, 3, 1), (LINE, 4, 1),
     (LINE, 4, 0), (LINE, 5, 0), (LINE, 5, 1), (LINE, 6, 0), (LINE, 6, 1),
     (SCALE,),),
    ((FINAL,),),
    (),
    (),
    ((OVER, 4, 0), (OVER, 4, 1),),
    (),
    ((LAST, 0, 0), (LAST, 1, 0), (LAST, 1, 1), (CROSS, 0),),
    ((TURN,),),
    ((CROSS, 1), (OVER, 5, 0), (OVER, 5, 1), (LAST, 0, 1), (OVER, 6, 1),
     (OVER, 6, 0),),
    (),
    (),
)
IN_NEAR = (
    ((LINE, 0, 0), (LINE, 2, 0), (PASS, 0, 0), (LINE, 2, 1), (LINE, 0, 1),
     (PASS, 0, 1), (SHARE,), (OVER, 0, 0), (LINE, 1, 0), (OVER, 1, 0),
     (LINE, 1, 1), (OVER, 1, 1), (OVER, 0, 1), (TOKENS,), (SUM, 0), (SUM, 1),
     (PASS, 1, 1), (LINE, 3, 0), (OVER, 3, 0), (PASS, 1, 0), (LINE, 4, 0),
     (SUM, 2), (LINE, 3, 1), (OVER, 2, 0), (OVER, 2, 1), (OVER, 3, 1),
     (LINE, 4, 1), (LINE, 5, 0), (LINE, 5, 1), (LINE, 6, 0), (LINE, 6, 1),
     (SCALE,),),
    (),
    (),
    (),
    (),
    ((LAST, 0, 1),),
    ((LAST, 0, 0), (LAST, 1, 0), (LAST, 1, 1), (CROSS, 0),),
    (),
    ((OVER, 4, 0), (OVER, 4, 1), (CROSS, 1), (OVER, 5, 0), (OVER, 5, 1),
     (OVER, 6, 0), (OVER, 6, 1),),
    (),
    (),
)
IN_FAR = (
    ((PASS, 0, 1), (PASS, 1, 0), (PASS, 1, 1), (SHARE,), (TOKENS,), (SUM, 0),
     (SUM, 2), (SUM, 1), (SCALE,), (PASS, 0, 0), (LINE, 0, 0), (OVER, 0, 0),
     (LINE, 0, 1), (OVER, 0, 1),),
    ((LINE, 2, 0), (OVER, 2, 0),),
    ((LINE, 2, 1), (OVER, 2, 1),),
    ((LINE, 4, 0),),
    ((LINE, 1, 0), (LINE, 4, 1), (OVER, 1, 0), (LINE, 1, 1), (OVER, 1, 1),),
    ((LINE, 5, 0), (LINE, 5, 1), (OVER, 4, 0),),
    ((LINE, 6, 0), (LINE, 6, 1), (LAST, 0, 0), (LAST, 0, 1), (LINE, 3, 0),
     (OVER, 3, 0), (LINE, 3, 1), (OVER, 3, 1), (CROSS, 0),),
    ((OVER, 4, 1),),
    ((LAST, 1, 0), (CROSS, 1), (OVER, 5, 0), (OVER, 5, 1), (OVER, 6, 0),
     (OVER, 6, 1),),
    ((LAST, 1, 1),),
    (),
)


def kernel(
    n, n_tp,
    tokens_hbm, gain_hbm, upm_hbm, downm_hbm,
    up, down, own, take, crossed,
    gain_in, upm_in, downm_in, tok, shard, passing, scale, sums, hidden, kept, give, cross,
    tok_recv, gather_recv, up_send, upz_recv, upy_recv, both_recv,
    down_send, downz_recv, downy_recv, pass_send, pass_recv, last_recv,
    pair_recv, cross_recv, once_send, local_sem,
):
    f32, bf16 = jnp.float32, jnp.bfloat16
    f, t = lax.axis_index("fs"), lax.axis_index("tp")
    lines = n // 2
    z, y = f // 2, f % 2
    t1 = t + 1 - 2 * (t % 2)
    t2 = (t + 2) % 4
    t3 = (t1 + 2) % 4
    members = n // n_tp
    starts = members // 2
    owner = f // members
    above, below = (f + 2) % n, (f + n - 2) % n
    across = f + 1 - 2 * y
    has_above, has_below = z < lines - 1, z > 0
    upper, lower = t >= n_tp // 2, t < n_tp // 2
    at_end = jnp.logical_not(has_above & has_below)

    up_rows = upm_in.shape[0]
    down_rows = downm_in.shape[0]
    rows_all, feats = tokens_hbm.shape
    half = feats // 2
    width = up.shape[1]
    (up_over, down_over_send, last_over, gather_send, tok_send, pair_send, cross_send) = (
        once_send.at[i] for i in range(7)
    )
    dcut = down_rows // DOWN_CUTS
    first_cut = max(8, up_rows * BOTH // 128 * 8)
    ucuts = (first_cut, first_cut + (up_rows - first_cut) // 16 * 8, up_rows)

    def remote(src, dst, send, recv, **to):
        return pltpu.make_async_remote_copy(
            src_ref=src, dst_ref=dst, send_sem=send, recv_sem=recv,
            device_id=to, device_id_type=pl.DeviceIdType.MESH,
        )

    def down_block(source, column):
        rows = pl.ds(pl.multiple_of(source % members * down_rows, down_rows), down_rows)
        return down.at[rows, pl.ds(pl.multiple_of(column * feats, feats), feats)]

    loads = [
        pltpu.make_async_copy(upm_hbm, upm_in, local_sem.at[0]),
        pltpu.make_async_copy(gain_hbm, gain_in.at[0], local_sem.at[1]),
        pltpu.make_async_copy(downm_hbm, downm_in, local_sem.at[2]),
        pltpu.make_async_copy(
            tokens_hbm, tok.at[:, pl.ds(pl.multiple_of(t * feats, feats), feats)],
            local_sem.at[3],
        ),
    ]
    for load in loads:
        load.start()

    barrier = pltpu.get_barrier_semaphore()
    for other in (t1, t2, t3):
        pl.semaphore_signal(
            barrier, inc=1, device_id={"tp": other}, device_id_type=pl.DeviceIdType.MESH
        )
    pl.semaphore_signal(
        barrier, inc=1, device_id={"fs": across}, device_id_type=pl.DeviceIdType.MESH
    )

    @pl.when(has_above)
    def _():
        pl.semaphore_signal(
            barrier, inc=1, device_id={"fs": above}, device_id_type=pl.DeviceIdType.MESH
        )

    @pl.when(has_below)
    def _():
        pl.semaphore_signal(
            barrier, inc=1, device_id={"fs": below}, device_id_type=pl.DeviceIdType.MESH
        )

    loads[0].wait()
    loads[1].wait()
    gain = jnp.transpose(jnp.broadcast_to(gain_in[...], (LANES, up_rows)))
    for first in range(0, up.shape[1], LANES):
        up[pl.ds(pl.multiple_of(f * up_rows, up_rows), up_rows), pl.ds(first, LANES)] = (
            gain * upm_in[:, pl.ds(first, LANES)]
        ).astype(bf16)

    loads[2].wait()

    @pl.when(owner == t)
    def _():
        down_block(f, t)[...] = downm_in[...].astype(bf16)

    @pl.when(owner == t2)
    def _():
        passing[z % starts] = downm_in[...].astype(bf16)

    @pl.when((owner == t1) | (owner == t3))
    def _():
        shard[...] = downm_in[...].astype(bf16)

    pl.semaphore_wait(
        barrier, 4 + has_above.astype(jnp.int32) + has_below.astype(jnp.int32)
    )

    def up_piece(line, column, u):
        first, last = (ucuts[u], ucuts[u + 1]) if u >= 0 else (0, ucuts[0])
        row = (line * 2 + column) * up_rows + first
        return up.at[pl.ds(pl.multiple_of(row, 8), last - first), :]

    def both_copy(way, line, column, to):
        piece = up_piece(line, column, -1)
        return remote(
            piece, piece, up_over if way == 2 else up_send.at[way, line],
            both_recv.at[line, column], fs=to,
        )

    def spent(ref, send):
        remote(ref, ref, send, local_sem.at[0], fs=across).wait_send()

    def landed(ref, recv):
        remote(ref, ref, local_sem.at[0], recv, fs=across).wait_recv()

    def both_onward(line, column):
        @pl.when(has_above & (line <= z))
        def _():
            both_copy(0, line, column, above).start()

        @pl.when(has_below & (line >= z))
        def _():
            both_copy(1, line, column, below).start()

    def up_copy(way, line, u, to):
        piece = up_piece(line, y, u)
        if way == 2:
            return remote(piece, piece, up_over, upy_recv.at[line // starts], fs=to)
        return remote(piece, piece, up_send.at[way, line], upz_recv.at[line, u], fs=to)

    def up_onward(line, u):
        @pl.when(has_above & (line <= z))
        def _():
            up_copy(0, line, u, above).start()

        @pl.when(has_below & (line >= z))
        def _():
            up_copy(1, line, u, below).start()

        up_copy(2, line, u, across).start()

    both_copy(2, z, y, across).start()
    for u in range(UP_CUTS):
        up_onward(z, u)
    both_onward(z, y)

    def gather_copy(column, to):
        return remote(
            shard, down_block(f, column), gather_send, gather_recv.at[column], tp=to
        )

    order = ((t3, 0), (t2, 0), (t3, 1), (t2, 1), (t1, 0), (t1, 1), (t, 0), (t, 1))
    passed = (1, 3)
    finals = 7
    early = (0, 1, 2)

    passes_down = lower & has_below
    passes_up = upper & has_above

    def pass_copies(part, js, q, ways=(0, 1)):
        line = t2 * starts + js
        row = ((line * 2 + y) % members) * down_rows + q * dcut
        here = passing.at[js, pl.ds(q * dcut, dcut), pl.ds(part * half, half)]
        there = down.at[
            pl.ds(pl.multiple_of(row, dcut), dcut),
            pl.ds(pl.multiple_of(t * feats + part * half, half), half),
        ]

        def onward(to):
            remote(here, here, pass_send.at[0, js], pass_recv.at[part, js, q], fs=to).start()

        if 0 in ways:
            @pl.when(passes_down & (line >= z))
            def _():
                onward(below)

            @pl.when(passes_up & (line <= z))
            def _():
                onward(above)

        if 1 in ways:
            @pl.when((upper & (line <= z)) | (lower & (line >= z)))
            def _():
                remote(
                    here, there, pass_send.at[1, js], downz_recv.at[passed[part], js, q],
                    tp=t2,
                ).start()

    def pass_on(part, q):
        @pl.loop(0, starts)
        def _(js):
            line = t2 * starts + js

            @pl.when((upper & (line < z)) | (lower & (line > z)))
            def _():
                here = passing.at[js, pl.ds(q * dcut, dcut), pl.ds(part * half, half)]
                landed(here, pass_recv.at[part, js, q])
                pass_copies(part, js, q)

    def pass_start(way):
        @pl.when(owner == t2)
        def _():
            for part in range(2):
                for q in range(DOWN_CUTS):
                    pass_copies(part, z % starts, q, (way,))

    @pl.when((owner == t1) | (owner == t3))
    def _():
        gather_copy(t, owner).start()

    pass_start(1)
    loads[3].wait()

    def tok_copy(way, column, to):
        piece = tok.at[:, pl.ds(pl.multiple_of(column * feats, feats), feats)]
        return remote(piece, piece, tok_send, tok_recv.at[way], tp=to)

    tok_copy(1, t, t2).start()
    tok_copy(0, t, t1).start()

    sums[...] = jnp.zeros(sums.shape, f32)
    both_copy(2, z, 1 - y, across).wait_recv()
    both_onward(z, 1 - y)

    def both_relay(line, column):
        @pl.when((line >= 0) & (line < lines))
        def _():
            both_copy(0, line, column, above).wait_recv()
            both_onward(line, column)

    def down_piece(ci, js, side, q):
        column, part = order[ci]
        line = t * starts + js
        row = ((line * 2 + side) % members) * down_rows + q * dcut
        return down.at[
            pl.ds(pl.multiple_of(row, dcut), dcut),
            pl.ds(pl.multiple_of(column * feats + part * half, half), half),
        ]

    def down_copy(way, ci, js, q, to):
        piece = down_piece(ci, js, y, q)
        if way == 2:
            send = last_over if ci == finals else down_over_send
            return remote(piece, piece, send, downy_recv.at[ci], fs=to)
        return remote(piece, piece, down_send.at[way, js], downz_recv.at[ci, js, q], fs=to)

    def down_lines(ci, js, q):
        line = t * starts + js
        rising = has_above & (line <= z)
        falling = has_below & (line >= z)
        if ci in passed:
            rising = rising & upper
            falling = falling & lower
        else:
            rising = rising & (upper | (line < z))
            falling = falling & (lower | (line > z))

        @pl.when(rising)
        def _():
            down_copy(0, ci, js, q, above).start()

        @pl.when(falling)
        def _():
            down_copy(1, ci, js, q, below).start()

    def down_over(ci, js, q):
        if ci in early:
            @pl.when(t * starts + js != z)
            def _():
                down_copy(2, ci, js, q, across).start()
        else:
            down_copy(2, ci, js, q, across).start()

    def far_start():
        js = z % starts

        def send(make):
            @pl.when(lower & has_above)
            def _():
                make(0, above).start()

            @pl.when(upper & has_below)
            def _():
                make(1, below).start()

        @pl.when(owner == t)
        def _():
            for ci in (0, 2, 4, 5, 6):
                for q in range(DOWN_CUTS):
                    send(lambda way, to: down_copy(way, ci, js, q, to))
            for q in range(DOWN_CUTS):
                send(lambda way, to: last_copy(way, js, y, q, to))

    def last_copy(way, js, side, q, to):
        piece = down_piece(finals, js, side, q)
        return remote(
            piece, piece, down_send.at[way, js], last_recv.at[js, side, q], fs=to
        )

    def last_onward(js, side, q, sent=True):
        line = t * starts + js
        rising = has_above & (line <= z)
        falling = has_below & (line >= z)
        if sent:
            rising = rising & (upper | (line < z))
            falling = falling & (lower | (line > z))

        @pl.when(rising)
        def _():
            last_copy(0, js, side, q, above).start()

        @pl.when(falling)
        def _():
            last_copy(1, js, side, q, below).start()

    def relay(ci, q, ways=(0, 1)):
        @pl.loop(0, starts)
        def _(js):
            if 0 in ways or 2 in ways:
                if ci in passed and ci not in early:
                    down_copy(0, ci, js, q, above).wait_recv()
                else:
                    @pl.when(t * starts + js != z)
                    def _():
                        down_copy(0, ci, js, q, above).wait_recv()

            if 0 in ways:
                down_lines(ci, js, q)
            if 1 in ways:
                down_over(ci, js, q)

    def last_turn():
        @pl.when(owner == t)
        def _():
            js = z % starts
            landed(down.at[pl.ds(0, down_rows), pl.ds(0, half)], downy_recv.at[finals])
            for q in range(DOWN_CUTS):
                last_onward(js, 1 - y, q, False)
                last_onward(js, y, q)

    def last_relay(side, q):
        @pl.loop(0, starts)
        def _(js):
            @pl.when(t * starts + js != z)
            def _():
                last_copy(0, js, side, q, above).wait_recv()
                last_onward(js, side, q)

    def relayed(ci):
        landed(down.at[pl.ds(0, starts * down_rows), pl.ds(0, half)], downy_recv.at[ci])

    @pl.when(owner == t)
    def _():
        for ci in (4, 0):
            gather_copy(order[ci][0], t).wait_recv()

    @pl.when(at_end)
    def _():
        pass_start(0)
        far_start()

    step = min(rows_all, 128)
    low = (z < lines // 2).astype(jnp.int32)
    final = low * (n_tp - 1)

    inside = has_above & has_below
    near = (lower & (z < lines // 2)) | (upper & (z >= lines // 2))
    far = jnp.logical_not(near)

    def share():
        tok_copy(1, t2, t2).wait_recv()
        tok_copy(2, t2, t1).start()

    def scales():
        @pl.loop(0, rows_all // step)
        def _(i):
            rows = pl.ds(pl.multiple_of(i * step, step), step)
            values = tok[rows, :].astype(f32)
            mean_square = jnp.mean(values * values, axis=-1, keepdims=True)
            scale[rows, :] = lax.rsqrt(mean_square + 1e-06)

    def ordered(c):
        return low * c + (1 - low) * (n_tp - 1 - c)

    def reach(c):
        return ordered(c) * starts + starts - 1

    rest = up_rows - first_cut

    def arrived(c):
        landed(up.at[pl.ds(0, starts * rest), :], upy_recv.at[c])

    def before(c, columns):
        part = pl.ds(pl.multiple_of(c * feats, feats), feats)
        return jnp.dot(tok[:, part], up[part, columns], preferred_element_type=f32)

    def accumulate(c):
        arrived(c)

        @pl.loop(0, width // COLUMNS)
        def _(i):
            columns = pl.ds(pl.multiple_of(i * COLUMNS, COLUMNS), COLUMNS)
            sums[:, columns] += before(c, columns)

    def second():
        @pl.loop(0, n_tp)
        def _(c):
            @pl.when(reach(c) == lines - 2)
            def _():
                accumulate(c)

    @pl.loop(1, lines)
    def _(d):
        last = at_end & (d == lines - 1)

        def reached(c, step_c):
            @pl.loop(0, 2)
            def _(j):
                @pl.when(reach(c + j * step_c) <= lines - 3)
                def _():
                    accumulate(c + j * step_c)

        @pl.when(last)
        def _():
            tok_copy(0, t1, t1).wait_recv()
            reached(t, t1 - t)

        @pl.when(last & far)
        def _():
            share()
            tok_copy(2, t3, t1).wait_recv()
            reached(t2, t3 - t2)

        for u in range(UP_CUTS):
            @pl.when(z - d >= 0)
            def _():
                up_copy(0, z - d, u, above).wait_recv()
                up_onward(z - d, u)

            @pl.when(z + d < lines)
            def _():
                up_copy(1, z + d, u, below).wait_recv()
                up_onward(z + d, u)

            if u == 0:
                @pl.when(last & far)
                def _():
                    second()
                    scales()

                pl.when(last & near)(share)

            if u == UP_CUTS - 1:
                @pl.when(last & near)
                def _():
                    tok_copy(2, t3, t1).wait_recv()
                    scales()

        for column in (y, 1 - y):
            both_relay(z - d, column)
            both_relay(z + d, column)

        for k in range(len(early)):
            @pl.when((owner == t) & (d == k + 1))
            def _():
                for q in range(DOWN_CUTS):
                    if early[k] in passed:
                        down_copy(0, early[k], z % starts, q, above).wait_recv()
                    down_copy(2, early[k], z % starts, q, across).start()

    @pl.when(has_above & has_below)
    def _():
        pass_start(0)
        far_start()

    every = range(DOWN_CUTS)

    def final_over():
        for q in every:
            down_copy(2, finals, z % starts, q, across).start()

    def late_tokens():
        second()

    def all_tokens():
        tok_copy(0, t1, t1).wait_recv()
        tok_copy(2, t3, t1).wait_recv()

    def product(ci):
        column, part = order[ci]
        first = pl.multiple_of(column * feats + part * half, half)
        return jnp.dot(hidden[...], down[:, pl.ds(first, half)], preferred_element_type=f32)

    def pair_copy(i):
        return remote(give.at[i], take.at[i], pair_send, pair_recv.at[i], tp=t1)

    def cross_copy(i):
        return remote(cross.at[i], crossed.at[i], cross_send, cross_recv.at[i], tp=t2)

    def cross_over(i):
        pair_copy(i).wait_recv()

        @pl.loop(0, rows_all // step)
        def _(j):
            rows = pl.ds(pl.multiple_of(j * step, step), step)
            cross[i, rows, :] = (kept[rows, :] + take[i, rows, :].astype(f32)).astype(bf16)

        cross_copy(i).start()

    def line_in(ci, q, end):
        relay(ci, q, (2,) if end else (0,))

    actions = {
        LINE: line_in,
        OVER: lambda ci, q, end: relay(ci, q, (1,)),
        LAST: lambda side, q, end: last_relay(y + side - 2 * y * side, q),
        PASS: lambda part, q, end: pass_on(part, q),
        SHARE: lambda end: share(),
        TOKENS: lambda end: late_tokens() if end else all_tokens(),
        SUM: lambda c, end: accumulate(ordered(c)),
        SCALE: lambda end: scales(),
        FINAL: lambda end: final_over(),
        TURN: lambda end: last_turn(),
        CROSS: lambda i, end: cross_over(i),
    }
    own_line = owner == t
    other_line = owner != t
    kinds = (
        (at_end & near & own_line, END_OWN), (at_end & near & other_line, END_NEAR),
        (at_end & far, END_FAR), (inside & near & own_line, IN_OWN),
        (inside & near & other_line, IN_NEAR), (inside & far, IN_FAR),
    )

    def slot(s):
        for kind, (condition, plan) in enumerate(kinds):
            def moves():
                for move, *args in plan[s]:
                    actions[move](*args, kind < 3)

            if plan[s]:
                pl.when(condition)(moves)

    slot(0)
    arrived(final)
    tiles = width // COLUMNS
    steps = 4
    for k in range(steps):
        @pl.loop(k * tiles // steps, (k + 1) * tiles // steps)
        def _(i):
            columns = pl.ds(pl.multiple_of(i * COLUMNS, COLUMNS), COLUMNS)
            value = jnp.maximum((sums[:, columns] + before(final, columns)) * scale[...], 0.0)
            hidden[:, columns] = (value * value).astype(bf16)

        slot(k + 1)

    def drain():
        @pl.loop(0, lines)
        def _(line):
            for way, onward in ((0, has_above & (line <= z)), (1, has_below & (line >= z))):
                @pl.when(onward)
                def _():
                    spent(up.at[pl.ds(0, up_rows + first_cut), :], up_send.at[way, line])

        spent(up.at[pl.ds(0, lines * rest + first_cut), :], up_over)

        @pl.loop(0, starts)
        def _(js):
            line = t2 * starts + js

            @pl.when((passes_down & (line >= z)) | (passes_up & (line <= z)))
            def _():
                spent(passing.at[js], pass_send.at[0, js])

            @pl.when((upper & (line <= z)) | (lower & (line >= z)))
            def _():
                spent(passing.at[js], pass_send.at[1, js])

        @pl.when((owner == t1) | (owner == t3))
        def _():
            spent(shard, gather_send)

        spent(tok.at[:, pl.ds(0, 3 * feats)], tok_send)

    def drain_down():
        @pl.loop(0, starts)
        def _(js):
            line = t * starts + js
            for way, onward, most in (
                (0, has_above & (line <= z), upper), (1, has_below & (line >= z), lower),
            ):
                for condition, pieces in ((most, 9), (jnp.logical_not(most), 7)):
                    @pl.when(onward & condition)
                    def _():
                        amount = pieces * down_rows // 8
                        spent(tok.at[pl.ds(0, amount), :], down_send.at[way, js])

        spent(down.at[pl.ds(0, starts * down_rows), pl.ds(0, 7 * half)], down_over_send)

        @pl.when(owner == t)
        def _():
            spent(down.at[pl.ds(0, down_rows), pl.ds(0, half)], last_over)

    relayed(0)
    give[0] = product(0).astype(bf16)
    pair_copy(0).start()
    slot(5)
    relayed(1)
    kept[...] = product(1)
    slot(6)
    relayed(2)
    give[1] = product(2).astype(bf16)
    pair_copy(1).start()
    slot(7)
    relayed(3)
    kept[...] = product(3)
    slot(8)
    relayed(4)
    give[2] = product(4).astype(bf16)
    pair_copy(2).start()
    slot(9)
    relayed(5)
    give[3] = product(5).astype(bf16)
    pair_copy(3).start()
    slot(10)
    drain()
    own[1] = product(7)
    if down_rows % LANES == 0:
        def partly(side):
            def term(js):
                part = pl.ds(
                    pl.multiple_of((2 * js + side) * down_rows, down_rows), down_rows
                )
                first = pl.multiple_of(t * feats, feats)
                return jnp.dot(
                    hidden[:, part], down[part, pl.ds(first, half)],
                    preferred_element_type=f32,
                )

            return sum((term(js) for js in range(1, starts)), term(0))

        own[0] = partly(y)
        relayed(6)
        own[0] += partly(1 - y)
    else:
        relayed(6)
        own[0] = product(6)
    for i in range(2):
        pair_copy(2 + i).wait_recv()
        cross_copy(i).wait_recv()

    drain_down()
    spent(give, pair_send)
    spent(cross, cross_send)


def finish(up, down, own, take, crossed, mixed_hbm, up_hbm, down_hbm, mixed, sems):
    copies = [
        pltpu.make_async_copy(up, up_hbm, sems.at[0]),
        pltpu.make_async_copy(down, down_hbm, sems.at[1]),
    ]
    for copy in copies:
        copy.start()
    rows_all, half = own.shape[1:]
    step = min(rows_all, 128)
    for i in range(2):
        @pl.loop(0, rows_all // step)
        def _(j):
            rows = pl.ds(pl.multiple_of(j * step, step), step)
            mixed[rows, pl.ds(i * half, half)] = (
                own[i, rows, :] + take[2 + i, rows, :].astype(jnp.float32)
                + crossed[i, rows, :].astype(jnp.float32)
            ).astype(mixed.dtype)

    copies.append(pltpu.make_async_copy(mixed, mixed_hbm, sems.at[2]))
    copies[2].start()
    for copy in copies:
        copy.wait()


def fused(n, n_tp, tokens, norm_gain, up_master, down_master):
    rows, feats = tokens.shape
    up_rows, width = up_master.shape
    down_rows = down_master.shape[0]
    depth = up_rows * n
    model = feats * n_tp
    half = feats // 2
    lines, starts = n // 2, n // n_tp // 2
    bf16, f32 = jnp.bfloat16, jnp.float32
    dma = pltpu.SemaphoreType.DMA
    vmem = pl.BlockSpec(memory_space=pltpu.VMEM)
    hbm = pl.BlockSpec(memory_space=pltpu.HBM)
    flops = 4 * rows * depth * width
    kept = pl.pallas_call(
        functools.partial(kernel, n, n_tp),
        out_shape=(
            pltpu.VMEM((depth, width), bf16),
            pltpu.VMEM((width, model), bf16),
            pltpu.VMEM((2, rows, half), f32),
            pltpu.VMEM((4, rows, half), bf16),
            pltpu.VMEM((2, rows, half), bf16),
        ),
        in_specs=[hbm] * 4,
        out_specs=(vmem,) * 5,
        scratch_shapes=[
            pltpu.VMEM((1, up_rows), f32),
            pltpu.VMEM(up_master.shape, f32),
            pltpu.VMEM(down_master.shape, f32),
            pltpu.VMEM((rows, model), bf16),
            pltpu.VMEM((down_rows, feats), bf16),
            pltpu.VMEM((starts, down_rows, feats), bf16),
            pltpu.VMEM((rows, 1), f32),
            pltpu.VMEM((rows, width), f32),
            pltpu.VMEM((rows, width), bf16),
            pltpu.VMEM((rows, half), f32),
            pltpu.VMEM((4, rows, half), bf16),
            pltpu.VMEM((2, rows, half), bf16),
            dma((3,)), dma((n_tp,)),
            dma((2, lines)), dma((lines, UP_CUTS)), dma((n_tp,)), dma((lines, 2)),
            dma((2, starts)), dma((8, starts, DOWN_CUTS)), dma((8,)),
            dma((2, starts)), dma((2, starts, DOWN_CUTS)), dma((starts, 2, DOWN_CUTS)),
            dma((4,)), dma((2,)), dma((7,)), dma((4,)),
        ],
        compiler_params=pltpu.CompilerParams(
            collective_id=0, has_side_effects=True, vmem_limit_bytes=VMEM_LIMIT * MIB
        ),
        cost_estimate=pl.CostEstimate(flops=flops, bytes_accessed=16 * MIB, transcendentals=0),
        name="layer",
    )(tokens, norm_gain, up_master, down_master)
    return pl.pallas_call(
        finish,
        out_shape=(
            jax.ShapeDtypeStruct((rows, feats), bf16),
            jax.ShapeDtypeStruct((depth, width), bf16),
            jax.ShapeDtypeStruct((width, model), bf16),
        ),
        in_specs=[vmem] * 5,
        out_specs=(hbm,) * 3,
        scratch_shapes=[pltpu.VMEM((rows, feats), bf16), dma((3,))],
        compiler_params=pltpu.CompilerParams(vmem_limit_bytes=8 * MIB),
        name="finish",
    )(*kept)


def solution(mesh):
    n, n_tp = mesh.shape["fs"], mesh.shape["tp"]
    return jax.shard_map(
        functools.partial(fused, n, n_tp),
        mesh=mesh,
        in_specs=(P("fs", "tp"), P("fs"), P("fs", "tp"), P("fs", "tp")),
        out_specs=(P("fs", "tp"), P(None, "tp"), P("tp", None)),
        check_vma=False,
    )
```
